32 devices in a mesh: sp: 8 (over z, y), tp: 4 (over x, core).
Axes of the slice: x: 2, y: 2, z: 4, core: 2. Of those that a mesh axis runs over, the one named last changes fastest.
Arguments:
- latent: bfloat16 [2048, 2048], P('sp'), may hold values from -6 to 6
- context: bfloat16 [512, 2048], P('sp'), may hold values from -6 to 6
- condition: float32 [2048], P('sp'), may hold values from -6 to 6
- ctx_condition: float32 [2048], P('sp'), may hold values from -6 to 6
- shift_weight: bfloat16 [2048, 2048], P('sp', 'tp'), may hold values from -0.125 to 0.125
- scale_weight: bfloat16 [2048, 2048], P('sp', 'tp'), may hold values from -0.125 to 0.125
- gate_weight: bfloat16 [2048, 2048], P('sp', 'tp'), may hold values from -0.125 to 0.125
- norm_gain: float32 [2048], replicated, may hold values from 0.1 to 1.9
- query_weight: bfloat16 [2048, 1024], P(None, 'tp'), may hold values from -0.125 to 0.125
- key_weight: bfloat16 [2048, 1024], P(None, 'tp'), may hold values from -0.125 to 0.125
- value_weight: bfloat16 [2048, 1024], P(None, 'tp'), may hold values from -0.125 to 0.125
- query_gain: float32 [64], replicated, may hold values from 0.6 to 6.5
- key_gain: float32 [64], replicated, may hold values from 0.6 to 6.5
- offset_bias: float32 [16, 15, 31], P('tp'), may hold values from 1 to 3
- out_weight: bfloat16 [1024, 2048], P('tp'), may hold values from -0.75 to 0.75
Outputs:
- mixed_rows: bfloat16 [2048, 2048], P('sp')
The draws below stay inside these ranges and needn't reach their ends.
All inputs are finite; a program needn't handle non-finite values.
Results may differ from the reference program's by a relative error of at most 0.01405.
The reference program's roundings to bfloat16 on the way count: a program that leaves them out, or rounds other values in their place, can miss the bound.
Values may be sent and summed in bfloat16 or wider, within the bound.
A program may use at most 64 MiB of HBM per device.

```python
import jax
import jax.numpy as jnp
from jax import lax

D = 2048
HEADS = 16
HEAD_DIM = 64
GRID_W = 64
WIN_ROWS = 8
WIN_COLS = 16
CTX = 512
TOKENS = 2048
ATT_W = 1024
N_TP = 4


def gain_draw(base_key):
    return jax.random.uniform(base_key, (HEAD_DIM,), jnp.float32, 0.6, 2.0)


def draw_query_gain(key, part):
    return gain_draw(jax.random.fold_in(key, 11))


def draw_key_gain(key, part):
    return gain_draw(jax.random.fold_in(key, 23))


def level_of(stream_key, dims, cuts, smallest, largest):
    gain = 1.0
    for dim, shards_of in cuts:
        heights = jax.random.uniform(jax.random.fold_in(jax.random.fold_in(stream_key, 6), dim), (shards_of,), jnp.float32, smallest / len(cuts), largest / len(cuts))
        gain = gain * jnp.repeat(jnp.exp(heights), dims[dim] // shards_of).reshape((-1,) + (1,) * (len(dims) - 1 - dim))
    return gain


def gaussian(rng, extent, width, most, cuts=(), kind=jnp.bfloat16):
    values = width * jax.random.normal(rng, extent, jnp.float32)
    if cuts:
        values = values * level_of(rng, extent, cuts, -0.22, 0.18)
    return jnp.clip(values, -most, most).astype(kind)


def setup_inputs(seed: int = 0) -> dict:
    streams_of = jax.random.split(jax.random.key(seed), 16)
    latent = gaussian(streams_of[0], (TOKENS, D), 1.0, 6.0, ((0, 8),))
    context = gaussian(streams_of[1], (CTX, D), 1.0, 6.0, ((0, 8),))
    condition = gaussian(streams_of[2], (D,), 1.0, 6.0, ((0, 8),), jnp.float32)
    ctx_condition = gaussian(streams_of[3], (D,), 1.0, 6.0, ((0, 8),), jnp.float32)
    shift_weight = gaussian(streams_of[4], (D, D), D ** -0.5, 0.125, ((0, 8), (1, 4)))
    scale_weight = gaussian(streams_of[5], (D, D), D ** -0.5, 0.125, ((0, 8), (1, 4)))
    gate_weight = gaussian(streams_of[6], (D, D), D ** -0.5, 0.125, ((0, 8), (1, 4)))
    norm_gain = jnp.clip(1.0 + 0.18 * jax.random.normal(streams_of[7], (D,), jnp.float32), 0.1, 1.9)
    query_weight = gaussian(streams_of[8], (D, ATT_W), D ** -0.5, 0.125, ((1, 4),))
    key_weight = gaussian(streams_of[9], (D, ATT_W), D ** -0.5, 0.125, ((1, 4),))
    value_weight = gaussian(streams_of[10], (D, ATT_W), D ** -0.5, 0.125, ((1, 4),))
    query_gain = draw_query_gain(jax.random.fold_in(streams_of[15], 71), 0)
    key_gain = draw_key_gain(jax.random.fold_in(streams_of[15], 71), 0)
    offset_bias = jnp.clip(1.0 + 2.0 * jax.random.uniform(streams_of[13], (HEADS, 2 * WIN_ROWS - 1, 2 * WIN_COLS - 1), jnp.float32) ** level_of(streams_of[13], (HEADS, 2 * WIN_ROWS - 1, 2 * WIN_COLS - 1), ((0, 4),), -0.2, 0.2), 1.0, 3.0)
    out_weight = gaussian(streams_of[14], (ATT_W, D), (ATT_W // 16) ** -0.5, 0.75, ((0, 4),))
    return dict(latent=latent, context=context, condition=condition, ctx_condition=ctx_condition, shift_weight=shift_weight, scale_weight=scale_weight, gate_weight=gate_weight, norm_gain=norm_gain, query_weight=query_weight, key_weight=key_weight, value_weight=value_weight, query_gain=query_gain, key_gain=key_gain, offset_bias=offset_bias, out_weight=out_weight)


EPS = 1e-06

def modulate(rows_in, norm_gain, shift_vec, scale_vec):
    values = rows_in.astype(jnp.float32)
    normed = values * lax.rsqrt(lax.optimization_barrier(jnp.mean(values * values, axis=-1, keepdims=True)) + EPS)
    return (normed * norm_gain * (1.0 + scale_vec) + shift_vec).astype(jnp.bfloat16)

def head_norm(projected, head_gain):
    row_count = projected.shape[0]
    split_heads = projected.reshape(row_count, -1, head_gain.shape[0])
    normed = split_heads * lax.rsqrt(lax.optimization_barrier(jnp.mean(split_heads * split_heads, axis=-1, keepdims=True)) + EPS)
    return (normed * head_gain).astype(jnp.bfloat16).reshape(row_count, -1)

def per_head(matrix, row_count):
    return matrix.reshape(row_count, HEADS, HEAD_DIM).transpose(1, 0, 2)

def reference(latent, context, condition, ctx_condition, shift_weight, scale_weight, gate_weight, norm_gain, query_weight, key_weight, value_weight, query_gain, key_gain, offset_bias, out_weight):
    activations = jax.nn.silu(jnp.stack([condition, ctx_condition])).astype(jnp.bfloat16)
    shift_vec = jnp.dot(activations, shift_weight, preferred_element_type=jnp.float32)
    scale_vec = jnp.dot(activations, scale_weight, preferred_element_type=jnp.float32)
    gate_vec = jnp.dot(activations[:1], gate_weight, preferred_element_type=jnp.float32)
    hidden = modulate(latent, norm_gain, shift_vec[0], scale_vec[0])
    ctx_hidden = modulate(context, norm_gain, shift_vec[1], scale_vec[1])
    queries = head_norm(jnp.dot(hidden, query_weight, preferred_element_type=jnp.float32), query_gain)
    keys_lat = head_norm(jnp.dot(hidden, key_weight, preferred_element_type=jnp.float32), key_gain)
    values_lat = jnp.dot(hidden, value_weight, preferred_element_type=jnp.float32).astype(jnp.bfloat16)
    ctx_keys = head_norm(jnp.dot(ctx_hidden, key_weight, preferred_element_type=jnp.float32), key_gain)
    ctx_values = jnp.dot(ctx_hidden, value_weight, preferred_element_type=jnp.float32).astype(jnp.bfloat16)
    grid_rows = TOKENS // GRID_W
    score_scale = HEAD_DIM ** (-0.5)
    row_ids = jnp.arange(grid_rows, dtype=jnp.int32)
    band_start = jnp.clip(row_ids - WIN_ROWS // 2, 0, grid_rows - WIN_ROWS)
    band_rows = band_start[:, None] + jnp.arange(WIN_ROWS, dtype=jnp.int32)[None, :]
    row_steps = band_rows - row_ids[:, None] + WIN_ROWS - 1
    column_ids = jnp.arange(GRID_W, dtype=jnp.int32)
    col_start = jnp.clip(column_ids - WIN_COLS // 2, 0, GRID_W - WIN_COLS)
    col_open = (column_ids[None, :] >= col_start[:, None]) & (column_ids[None, :] < col_start[:, None] + WIN_COLS)
    col_steps = jnp.clip(column_ids[None, :] - column_ids[:, None], 1 - WIN_COLS, WIN_COLS - 1) + WIN_COLS - 1

    def one_head(operands):
        q_head, k_head, v_head, kc_head, vc_head, table = operands
        q_grid = q_head.reshape(grid_rows, GRID_W, HEAD_DIM).astype(jnp.float32)
        k_grid = k_head.reshape(grid_rows, GRID_W, HEAD_DIM).astype(jnp.float32)
        v_grid = v_head.reshape(grid_rows, GRID_W, HEAD_DIM).astype(jnp.float32)
        k_band = k_grid[band_rows]
        v_band = v_grid[band_rows]
        offsets = table[row_steps[:, None, :, None], col_steps[None, :, None, :]]
        local_scores = jnp.einsum('rqd,rjkd->rqjk', q_grid, k_band) * score_scale + offsets
        local_scores = jnp.where(col_open[None, :, None, :], local_scores, -jnp.inf)
        ctx_scores = jnp.einsum('rqd,nd->rqn', q_grid, kc_head.astype(jnp.float32)) * score_scale
        row_max = jnp.maximum(lax.optimization_barrier(jnp.max(local_scores, axis=(2, 3))), lax.optimization_barrier(jnp.max(ctx_scores, axis=2)))
        local_exp = jnp.exp(local_scores - row_max[..., None, None])
        ctx_exp = jnp.exp(ctx_scores - row_max[..., None])
        denominator = lax.optimization_barrier(jnp.sum(local_exp, axis=(2, 3))) + lax.optimization_barrier(jnp.sum(ctx_exp, axis=2))
        local_weights = (local_exp / denominator[..., None, None]).astype(jnp.bfloat16)
        ctx_weights = (ctx_exp / denominator[..., None]).astype(jnp.bfloat16)
        result = jnp.einsum('rqjk,rjkd->rqd', local_weights.astype(jnp.float32), v_band) + jnp.einsum('rqn,nd->rqd', ctx_weights.astype(jnp.float32), vc_head.astype(jnp.float32))
        return result.astype(jnp.bfloat16)
    attended = lax.map(one_head, (per_head(queries, TOKENS), per_head(keys_lat, TOKENS), per_head(values_lat, TOKENS), per_head(ctx_keys, CTX), per_head(ctx_values, CTX), offset_bias))
    attended = attended.transpose(1, 2, 0, 3).reshape(TOKENS, ATT_W)
    group_cols = ATT_W // N_TP
    branch = jnp.zeros((TOKENS, D), jnp.float32)
    for group in range(N_TP):
        partial_value = jnp.dot(attended[:, group * group_cols:(group + 1) * group_cols], out_weight[group * group_cols:(group + 1) * group_cols], preferred_element_type=jnp.float32)
        rounded = lax.optimization_barrier(partial_value.astype(jnp.bfloat16))
        branch = branch + rounded.astype(jnp.float32)
    return (latent.astype(jnp.float32) + gate_vec[0] * branch).astype(jnp.bfloat16)
```

```python
import functools

import jax
import jax.numpy as jnp
from jax import lax
from jax.experimental import pallas as pl
from jax.experimental.pallas import tpu as pltpu
from jax.sharding import PartitionSpec as P

HEAD_DIM = 64
GRID_W = 64
WIN_ROWS = 8
WIN_COLS = 16


EPS = 1e-06


def extended(x, sides, width):
    for axis, dim in sides:
        count, length = (lax.axis_size(axis), x.shape[dim])
        up = [(i, (i + 1) % count) for i in range(count - 1)]
        down = [(j, i) for i, j in up]
        last = lax.slice_in_dim(x, length - width, length, axis=dim)
        initial = lax.slice_in_dim(x, 0, width, axis=dim)
        before = lax.ppermute(last, axis, up)
        after = lax.ppermute(initial, axis, down)
        x = jnp.concatenate([before, x, after], axis=dim)
    return x


def modulate(rows_in, norm_gain, shift_vec, scale_vec):
    values = rows_in.astype(jnp.float32)
    normed = values * lax.rsqrt(jnp.mean(values * values, axis=-1, keepdims=True) + EPS)
    return (normed * norm_gain * (1.0 + scale_vec) + shift_vec).astype(jnp.bfloat16)


def head_norm(projected, head_gain):
    row_count = projected.shape[0]
    split_heads = projected.reshape(row_count, -1, head_gain.shape[0])
    normed = split_heads * lax.rsqrt(
        jnp.mean(split_heads * split_heads, axis=-1, keepdims=True) + EPS
    )
    return (normed * head_gain).astype(jnp.bfloat16).reshape(row_count, -1)


def per_device_plain(
    latent,
    context,
    condition,
    ctx_condition,
    shift_weight,
    scale_weight,
    gate_weight,
    norm_gain,
    query_weight,
    key_weight,
    value_weight,
    query_gain,
    key_gain,
    offset_bias,
    out_weight,
):
    activations = jax.nn.silu(jnp.stack([condition, ctx_condition])).astype(jnp.bfloat16)
    part_shift = jnp.dot(activations, shift_weight, preferred_element_type=jnp.float32)
    part_scale = jnp.dot(activations, scale_weight, preferred_element_type=jnp.float32)
    part_gate = jnp.dot(activations[:1], gate_weight, preferred_element_type=jnp.float32)
    block_cols = shift_weight.shape[1]
    first_col = lax.axis_index("tp") * block_cols

    def spread(piece_part):
        padded_vec = jnp.zeros((piece_part.shape[0], block_cols * lax.axis_size("tp")), jnp.float32)
        return lax.dynamic_update_slice_in_dim(padded_vec, piece_part, first_col, 1)

    shift_vec, scale_vec, gate_vec = lax.psum(
        (spread(part_shift), spread(part_scale), spread(part_gate)), ("sp", "tp")
    )
    hidden = modulate(latent, norm_gain, shift_vec[0], scale_vec[0])
    queries = head_norm(
        jnp.dot(hidden, query_weight, preferred_element_type=jnp.float32), query_gain
    )
    keys_lat = head_norm(jnp.dot(hidden, key_weight, preferred_element_type=jnp.float32), key_gain)
    values_lat = jnp.dot(hidden, value_weight, preferred_element_type=jnp.float32).astype(
        jnp.bfloat16
    )
    ctx_hidden = modulate(
        lax.all_gather(context, "sp", axis=0, tiled=True), norm_gain, shift_vec[1], scale_vec[1]
    )
    ctx_keys = head_norm(
        jnp.dot(ctx_hidden, key_weight, preferred_element_type=jnp.float32), key_gain
    )
    ctx_values = jnp.dot(ctx_hidden, value_weight, preferred_element_type=jnp.float32).astype(
        jnp.bfloat16
    )
    ctx_pairs = jnp.concatenate([ctx_keys, ctx_values], axis=1)
    col_width = keys_lat.shape[1]
    heads_dev = col_width // HEAD_DIM
    local_rows = keys_lat.shape[0] // GRID_W
    halo_rows = WIN_ROWS // 2
    window_keys = WIN_ROWS * GRID_W
    key_value = jnp.concatenate([keys_lat, values_lat], axis=1).reshape(
        local_rows, GRID_W, 2 * col_width
    )
    padded = extended(key_value, (("sp", 0),), halo_rows)
    first_row = lax.axis_index("sp") * local_rows
    total_rows = local_rows * lax.axis_size("sp")
    global_rows = first_row + jnp.arange(local_rows, dtype=jnp.int32)
    band_start = jnp.clip(global_rows - halo_rows, 0, total_rows - WIN_ROWS)
    band_global = band_start[:, None] + jnp.arange(WIN_ROWS, dtype=jnp.int32)[None, :]
    banded = jnp.take(padded, band_global - first_row + halo_rows, axis=0)
    key_band = banded[..., :col_width].reshape(local_rows, window_keys, heads_dev, HEAD_DIM)
    value_band = banded[..., col_width:].reshape(local_rows, window_keys, heads_dev, HEAD_DIM)
    row_steps = band_global - global_rows[:, None] + WIN_ROWS - 1
    row_hot = (
        row_steps[:, :, None] == jnp.arange(2 * WIN_ROWS - 1, dtype=jnp.int32)[None, None, :]
    ).astype(jnp.float32)
    column_ids = jnp.arange(GRID_W, dtype=jnp.int32)
    col_steps = (
        jnp.clip(column_ids[None, :] - column_ids[:, None], 1 - WIN_COLS, WIN_COLS - 1)
        + WIN_COLS
        - 1
    )
    col_hot = (
        col_steps[:, :, None] == jnp.arange(2 * WIN_COLS - 1, dtype=jnp.int32)[None, None, :]
    ).astype(jnp.float32)
    col_start = jnp.clip(column_ids - WIN_COLS // 2, 0, GRID_W - WIN_COLS)
    col_open = (column_ids[None, :] >= col_start[:, None]) & (
        column_ids[None, :] < col_start[:, None] + WIN_COLS
    )
    col_table = jnp.einsum("hab,qkb->haqk", offset_bias, col_hot, precision=lax.Precision.HIGHEST)
    col_table = jnp.where(col_open[None, None, :, :], col_table, -jnp.inf)
    offset_terms = jnp.einsum(
        "rja,haqk->hrqjk",
        row_hot,
        jnp.where(col_open[None, None], col_table, 0.0),
        precision=lax.Precision.HIGHEST,
    )
    offset_terms = jnp.where(col_open[None, None, :, None, :], offset_terms, -jnp.inf)
    offset_terms = offset_terms.reshape(heads_dev, local_rows, GRID_W, window_keys)
    score_scale = HEAD_DIM ** (-0.5)
    q_grid = queries.reshape(local_rows, GRID_W, heads_dev, HEAD_DIM)
    scores = (
        jnp.einsum("rqhd,rnhd->hrqn", q_grid, key_band, preferred_element_type=jnp.float32)
        * score_scale
        + offset_terms
    )
    ctx_count = ctx_pairs.shape[0]
    ctx_keys_all = ctx_pairs[:, :col_width].reshape(ctx_count, heads_dev, HEAD_DIM)
    ctx_values_all = ctx_pairs[:, col_width:].reshape(ctx_count, heads_dev, HEAD_DIM)
    ctx_scores = (
        jnp.einsum("rqhd,nhd->hrqn", q_grid, ctx_keys_all, preferred_element_type=jnp.float32)
        * score_scale
    )
    row_max = jnp.maximum(jnp.max(scores, axis=3), jnp.max(ctx_scores, axis=3))
    local_exp = jnp.exp(scores - row_max[..., None])
    ctx_exp = jnp.exp(ctx_scores - row_max[..., None])
    denominator = jnp.sum(local_exp, axis=3) + jnp.sum(ctx_exp, axis=3)
    local_weights = (local_exp / denominator[..., None]).astype(jnp.bfloat16)
    ctx_weights = (ctx_exp / denominator[..., None]).astype(jnp.bfloat16)
    combined = jnp.einsum(
        "hrqn,rnhd->rqhd", local_weights, value_band, preferred_element_type=jnp.float32
    ) + jnp.einsum(
        "hrqn,nhd->rqhd", ctx_weights, ctx_values_all, preferred_element_type=jnp.float32
    )
    attended = combined.astype(jnp.bfloat16).reshape(local_rows * GRID_W, col_width)
    partial_value = jnp.dot(attended, out_weight, preferred_element_type=jnp.float32)
    branch = lax.psum(partial_value.astype(jnp.bfloat16), "tp").astype(jnp.float32)
    return (latent.astype(jnp.float32) + gate_vec[0] * branch).astype(jnp.bfloat16)


MESH = pl.DeviceIdType.MESH
MASKED = -1e30
F32 = jnp.float32
BF16 = jnp.bfloat16


def fused_kernel(
    n_sp,
    n_tp,
    latent,
    context,
    shift_w,
    scale_w,
    gate_w,
    query_w,
    key_w,
    value_w,
    out_w,
    cond,
    ctx_cond,
    norm_gain,
    query_gain,
    key_gain,
    bias_rows,
    out,
    x_in,
    x_norm,
    hid,
    w_mod,
    w_qkv,
    w_out,
    mod_sp,
    mod_tp,
    q_s,
    k_all,
    v_all,
    ctx_k,
    ctx_v,
    table,
    att,
    local_sem,
    mod_send,
    mod_recv,
    modt_send,
    modt_recv,
    halo_send,
    halo_recv,
    ctx_send,
    ctx_recv,
    wo_send,
    wo_recv,
    att_send,
    att_recv,
):
    me_s, me_t = lax.axis_index("sp"), lax.axis_index("tp")
    rows, d = latent.shape
    c_rows = context.shape[0]
    width = key_w.shape[1]
    heads = width // HEAD_DIM
    block = shift_w.shape[1]
    l_rows = rows // GRID_W
    halo = WIN_ROWS // 2
    win = WIN_ROWS * GRID_W
    core = lax.rem(me_t, 2)
    chip = lax.div(me_t, 2)
    partner = me_t + 1 - 2 * core
    n_x = n_tp // 2

    def remote(src, dst, send, recv, s, t):
        return pltpu.make_async_remote_copy(
            src_ref=src, dst_ref=dst, send_sem=send, recv_sem=recv,
            device_id=(s, t), device_id_type=MESH,
        )

    barrier = pltpu.get_barrier_semaphore()
    for k in range(1, n_sp):
        pl.semaphore_signal(
            barrier, inc=1, device_id=(lax.rem(me_s + k, n_sp), me_t), device_id_type=MESH
        )
    for k in range(1, n_tp):
        pl.semaphore_signal(
            barrier, inc=1, device_id=(me_s, lax.rem(me_t + k, n_tp)), device_id_type=MESH
        )

    loads = [
        (shift_w, w_mod.at[0]),
        (scale_w, w_mod.at[1]),
        (gate_w, w_mod.at[2]),
        (context, x_in.at[pl.ds(0, c_rows)]),
        (latent, x_in.at[pl.ds(c_rows, rows)]),
        (key_w, w_qkv.at[0]),
        (value_w, w_qkv.at[1]),
        (query_w, w_qkv.at[2]),
        (out_w, w_out.at[me_t]),
    ]
    copies = [pltpu.make_async_copy(a, b, local_sem.at[i]) for i, (a, b) in enumerate(loads)]
    for c in copies:
        c.start()

    def silu(v):
        return v / (1.0 + jnp.exp(-v))

    two = (16, cond.shape[1])
    row_id = lax.broadcasted_iota(jnp.int32, two, 0)
    act0 = jnp.broadcast_to(silu(cond[...]), two)
    act1 = jnp.broadcast_to(silu(ctx_cond[...]), two)

    def placed(first, second):
        picked = jnp.where(row_id == first, act0, 0.0)
        if second is not None:
            picked = jnp.where(row_id == second, act1, picked)
        return picked.astype(BF16)

    part = jnp.zeros((16, block), F32)
    for i, (first, second) in enumerate(((0, 1), (2, 3), (4, None))):
        copies[i].wait()
        part += jnp.dot(placed(first, second), w_mod[i], preferred_element_type=F32)
    mod_sp[me_s] = part[:8]
    pl.semaphore_wait(barrier, n_sp + n_tp - 2)
    sends = []
    for k in range(1, n_sp):
        peer = lax.rem(me_s + k, n_sp)
        c = remote(
            mod_sp.at[me_s], mod_sp.at[me_s], mod_send.at[k], mod_recv.at[me_s], peer, me_t
        )
        c.start()
        sends.append(c)

    copies[3].wait()
    copies[4].wait()
    step = 32

    def norm_rows(i, carry):
        at = pl.ds(pl.multiple_of(i * step, step), step)
        v = x_in[at, :].astype(F32)
        r = lax.rsqrt(jnp.mean(v * v, axis=-1, keepdims=True) + EPS)
        x_norm[at, :] = v * r * norm_gain[...]
        return carry

    lax.fori_loop(0, (rows + c_rows) // step, norm_rows, 0)

    pair = 2 * GRID_W
    q_col = lax.broadcasted_iota(jnp.int32, (GRID_W, pair), 0)
    k_col = lax.broadcasted_iota(jnp.int32, (GRID_W, pair), 1) % GRID_W
    col0 = jnp.clip(q_col - WIN_COLS // 2, 0, GRID_W - WIN_COLS)
    col_open = (k_col >= col0) & (k_col < col0 + WIN_COLS)
    n_pairs = 2 * WIN_ROWS - 2
    for h in range(heads):
        for a in range(n_pairs):
            line = jnp.broadcast_to(bias_rows[h * n_pairs + a : h * n_pairs + a + 1, :], (GRID_W, pair))
            rolled = pltpu.roll(line, pair - (WIN_COLS - 1), 1, stride=1, stride_axis=0)
            table[a, h * GRID_W : (h + 1) * GRID_W, :] = jnp.where(col_open, rolled, MASKED)

    for k in range(1, n_sp):
        peer = lax.rem(me_s + k, n_sp)
        remote(
            mod_sp.at[peer], mod_sp.at[peer], mod_send.at[k], mod_recv.at[peer], peer, me_t
        ).wait_recv()
    total = mod_sp[0]
    for k in range(1, n_sp):
        total = total + mod_sp[k]
    mod_tp[me_t] = total
    for k in range(1, n_tp):
        peer = lax.rem(me_t + k, n_tp)
        c = remote(
            mod_tp.at[me_t], mod_tp.at[me_t], modt_send.at[k], modt_recv.at[me_t], me_s, peer
        )
        c.start()
        sends.append(c)

    def gather_start(buf, send, recv):
        started = [remote(buf.at[me_t], buf.at[me_t], send.at[0], recv.at[me_t], me_s, partner)]
        for k in range(1, n_x):
            far = 2 * lax.rem(chip + k, n_x) + core
            started.append(
                remote(buf.at[me_t], buf.at[me_t], send.at[k], recv.at[me_t], me_s, far)
            )
        for c in reversed(started):
            c.start()
        sends.extend(started)

    def gather_forward(buf, send, recv):
        for k in range(1, n_x):
            came = 2 * lax.rem(chip + n_x - k, n_x) + core
            c = remote(
                buf.at[came], buf.at[came], send.at[n_x + k], recv.at[came], me_s, partner
            )
            c.wait_recv()
            c.start()
            sends.append(c)

    def gather_finish(buf, send, recv):
        remote(
            buf.at[partner], buf.at[partner], send.at[0], recv.at[partner], me_s, partner
        ).wait_recv()
        for k in range(1, n_x):
            came = 2 * lax.rem(chip + n_x - k, n_x) + 1 - core
            remote(
                buf.at[came], buf.at[came], send.at[n_x + k], recv.at[came], me_s, partner
            ).wait_recv()

    for k in range(1, n_tp):
        peer = lax.rem(me_t + k, n_tp)
        remote(
            mod_tp.at[peer], mod_tp.at[peer], modt_send.at[k], modt_recv.at[peer], me_s, peer
        ).wait_recv()
    copies[8].wait()
    gather_start(w_out, wo_send, wo_recv)

    def vec(r):
        return jnp.concatenate([mod_tp[j][r : r + 1, :] for j in range(n_tp)], axis=1)

    def modulate_rows(first, count, shift, scale):
        def body(i, carry):
            at = pl.ds(pl.multiple_of(first + i * step, step), step)
            hid[at, :] = (x_norm[at, :] * scale + shift).astype(BF16)
            return carry

        lax.fori_loop(0, count // step, body, 0)

    modulate_rows(0, c_rows, vec(1), 1.0 + vec(3))
    modulate_rows(c_rows, rows, vec(0), 1.0 + vec(2))

    head_row = lax.broadcasted_iota(jnp.int32, (width, width), 0) // HEAD_DIM
    head_col = lax.broadcasted_iota(jnp.int32, (width, width), 1) // HEAD_DIM
    same_head = (head_row == head_col).astype(F32)

    def head_scale(p, gain):
        mean = jnp.dot(
            p * p, same_head, precision=lax.Precision.HIGHEST, preferred_element_type=F32
        ) * (1.0 / HEAD_DIM)
        return (p * lax.rsqrt(mean + EPS) * gain[...]).astype(BF16)

    last_s = n_sp - 1

    def share(index, value, block_all, block_ctx):
        block_ctx[me_s] = value[:c_rows]
        own = pl.ds(rows, rows)
        block_all[own, :] = value[c_rows:]
        up = remote(
            block_all.at[own], block_all.at[pl.ds(0, rows)],
            halo_send.at[index, 0], halo_recv.at[index, 0], me_s + 1, me_t,
        )
        down = remote(
            block_all.at[own], block_all.at[pl.ds(2 * rows, rows)],
            halo_send.at[index, 1], halo_recv.at[index, 1], me_s - 1, me_t,
        )

        @pl.when(me_s < last_s)
        def _():
            up.start()

        @pl.when(me_s > 0)
        def _():
            down.start()

        for k in range(1, n_sp):
            peer = lax.rem(me_s + k, n_sp)
            c = remote(
                block_ctx.at[me_s], block_ctx.at[me_s],
                ctx_send.at[index, k], ctx_recv.at[index, me_s], peer, me_t,
            )
            c.start()
            sends.append(c)
        return up, down

    copies[5].wait()
    keys = head_scale(jnp.dot(hid[...], w_qkv[0], preferred_element_type=F32), key_gain)
    halo_k = share(0, keys, k_all, ctx_k)
    copies[6].wait()
    values = jnp.dot(hid[...], w_qkv[1], preferred_element_type=F32).astype(BF16)
    halo_v = share(1, values, v_all, ctx_v)
    copies[7].wait()
    queries = head_scale(
        jnp.dot(hid[c_rows:, :], w_qkv[2], preferred_element_type=F32), query_gain
    )
    q_s[...] = queries * jnp.asarray(HEAD_DIM ** (-0.5), BF16)

    for up, down in (halo_k, halo_v):

        @pl.when(me_s > 0)
        def _():
            up.wait_recv()

        @pl.when(me_s < last_s)
        def _():
            down.wait_recv()

    for index, block_ctx in enumerate((ctx_k, ctx_v)):
        for k in range(1, n_sp):
            peer = lax.rem(me_s + k, n_sp)
            remote(
                block_ctx.at[peer], block_ctx.at[peer],
                ctx_send.at[index, k], ctx_recv.at[index, peer], peer, me_t,
            ).wait_recv()

    lane_head = lax.broadcasted_iota(jnp.int32, (GRID_W, width), 1) // HEAD_DIM
    masks = [(lane_head == h).astype(F32) for h in range(heads)]
    contract_last = (((1,), (1,)), ((), ()))
    all_ck = ctx_k[...].reshape(n_sp * c_rows, width)
    all_cv = ctx_v[...].reshape(n_sp * c_rows, width)
    for i in range(l_rows):
        start = jnp.where(me_s == 0, halo, jnp.where(me_s == last_s, 0, i))
        at = pl.ds(pl.multiple_of(start * GRID_W, GRID_W), win)
        qi = q_s[i * GRID_W : (i + 1) * GRID_W, :].astype(F32)
        qs = jnp.concatenate([(qi * m).astype(BF16) for m in masks], axis=0)
        s1 = lax.dot_general(qs, k_all[at, :], contract_last, preferred_element_type=F32)
        first = start - i + WIN_ROWS - 1 - halo
        s1 = s1 + jnp.concatenate([table[first + 2 * m] for m in range(WIN_ROWS // 2)], axis=1)
        s2 = lax.dot_general(qs, all_ck, contract_last, preferred_element_type=F32)
        top = jnp.maximum(
            jnp.max(s1, axis=1, keepdims=True), jnp.max(s2, axis=1, keepdims=True)
        )
        e1 = jnp.exp(s1 - top)
        e2 = jnp.exp(s2 - top)
        inv = 1.0 / (jnp.sum(e1, axis=1, keepdims=True) + jnp.sum(e2, axis=1, keepdims=True))
        o = jnp.dot((e1 * inv).astype(BF16), v_all[at, :], preferred_element_type=F32)
        o = o + jnp.dot((e2 * inv).astype(BF16), all_cv, preferred_element_type=F32)
        picked = o[:GRID_W] * masks[0]
        for h in range(1, heads):
            picked = picked + o[h * GRID_W : (h + 1) * GRID_W] * masks[h]
        att[me_t, i * GRID_W : (i + 1) * GRID_W, :] = picked.astype(BF16)

    gather_forward(w_out, wo_send, wo_recv)
    gather_start(att, att_send, att_recv)
    gather_forward(att, att_send, att_recv)
    gather_finish(w_out, wo_send, wo_recv)
    gather_finish(att, att_send, att_recv)
    gate = vec(4)
    cols = 512
    for n in range(d // cols):
        at = slice(n * cols, (n + 1) * cols)
        branch = jnp.zeros((rows, cols), F32)
        for j in range(n_tp):
            branch = branch + jnp.dot(
                att[j], w_out[j, :, at], preferred_element_type=F32
            ).astype(BF16).astype(F32)
        base = x_in[c_rows:, at].astype(F32)
        out[:, at] = (base + gate[:, at] * branch).astype(BF16)

    for c in sends:
        c.wait_send()
    for up, down in (halo_k, halo_v):

        @pl.when(me_s < last_s)
        def _():
            up.wait_send()

        @pl.when(me_s > 0)
        def _():
            down.wait_send()


def per_device(
    latent,
    context,
    condition,
    ctx_condition,
    shift_weight,
    scale_weight,
    gate_weight,
    norm_gain,
    query_weight,
    key_weight,
    value_weight,
    query_gain,
    key_gain,
    offset_bias,
    out_weight,
):
    n_sp, n_tp = lax.axis_size("sp"), lax.axis_size("tp")
    rows, d = latent.shape
    c_rows = context.shape[0]
    width = key_weight.shape[1]
    heads = width // HEAD_DIM
    block = shift_weight.shape[1]
    n_pairs = 2 * WIN_ROWS - 2
    padded = jnp.pad(offset_bias, ((0, 0), (0, 0), (0, GRID_W - offset_bias.shape[2])))
    bias_rows = jnp.concatenate([padded[:, :-1], padded[:, 1:]], axis=2).reshape(
        heads * n_pairs, 2 * GRID_W
    )
    any_spec = pl.BlockSpec(memory_space=pl.ANY)
    vmem_spec = pl.BlockSpec(memory_space=pltpu.VMEM)
    dma = pltpu.SemaphoreType.DMA
    return pl.pallas_call(
        functools.partial(fused_kernel, n_sp, n_tp),
        out_shape=jax.ShapeDtypeStruct((rows, d), BF16),
        in_specs=[any_spec] * 9 + [vmem_spec] * 6,
        out_specs=vmem_spec,
        scratch_shapes=[
            pltpu.VMEM((rows + c_rows, d), BF16),
            pltpu.VMEM((rows + c_rows, d), F32),
            pltpu.VMEM((rows + c_rows, d), BF16),
            pltpu.VMEM((3, shift_weight.shape[0], block), BF16),
            pltpu.VMEM((3, d, width), BF16),
            pltpu.VMEM((n_tp, width, d), BF16),
            pltpu.VMEM((n_sp, 8, block), F32),
            pltpu.VMEM((n_tp, 8, block), F32),
            pltpu.VMEM((rows, width), BF16),
            pltpu.VMEM((3 * rows, width), BF16),
            pltpu.VMEM((3 * rows, width), BF16),
            pltpu.VMEM((n_sp, c_rows, width), BF16),
            pltpu.VMEM((n_sp, c_rows, width), BF16),
            pltpu.VMEM((n_pairs, heads * GRID_W, 2 * GRID_W), F32),
            pltpu.VMEM((n_tp, rows, width), BF16),
            dma((9,)),
            dma((n_sp,)),
            dma((n_sp,)),
            dma((n_tp,)),
            dma((n_tp,)),
            dma((2, 2)),
            dma((2, 2)),
            dma((2, n_sp)),
            dma((2, n_sp)),
            dma((n_tp,)),
            dma((n_tp,)),
            dma((n_tp,)),
            dma((n_tp,)),
        ],
        compiler_params=pltpu.CompilerParams(collective_id=0, has_side_effects=True),
        name="fused_block",
    )(
        latent,
        context,
        shift_weight,
        scale_weight,
        gate_weight,
        query_weight,
        key_weight,
        value_weight,
        out_weight,
        condition.reshape(1, -1),
        ctx_condition.reshape(1, -1),
        norm_gain.reshape(1, -1),
        jnp.tile(query_gain, heads).reshape(1, -1),
        jnp.tile(key_gain, heads).reshape(1, -1),
        bias_rows,
    )


def fused_fits(latent, context, condition, query_weight, n_sp, n_tp):
    rows, c_rows = latent.shape[0] // n_sp, context.shape[0] // n_sp
    width = query_weight.shape[1] // n_tp
    return (
        rows == WIN_ROWS // 2 * GRID_W
        and c_rows % 32 == 0
        and condition.shape[0] // n_sp % 128 == 0
        and width % 128 == 0
        and n_tp % 2 == 0
        and n_sp > 1
    )


def solution(mesh):
    in_specs = (
        P("sp", None),
        P("sp", None),
        P("sp"),
        P("sp"),
        P("sp", "tp"),
        P("sp", "tp"),
        P("sp", "tp"),
        P(),
        P(None, "tp"),
        P(None, "tp"),
        P(None, "tp"),
        P(),
        P(),
        P("tp", None, None),
        P("tp", None),
    )
    out_specs = P("sp", None)

    def step(latent, context, condition, ctx_condition, *rest):
        n_sp, n_tp = mesh.shape["sp"], mesh.shape["tp"]
        fits = fused_fits(latent, context, condition, rest[4], n_sp, n_tp)
        body = per_device if fits else per_device_plain
        return jax.shard_map(
            body, mesh=mesh, in_specs=in_specs, out_specs=out_specs, check_vma=False
        )(latent, context, condition, ctx_condition, *rest)

    return step
```

```python
import functools

import jax
import jax.numpy as jnp
from jax import lax
from jax.experimental import pallas as pl
from jax.experimental.pallas import tpu as pltpu
from jax.sharding import PartitionSpec as P

HEAD_DIM = 64
GRID_W = 64
WIN_ROWS = 8
WIN_COLS = 16


EPS = 1e-06


def extended(x, sides, width):
    for axis, dim in sides:
        count, length = (lax.axis_size(axis), x.shape[dim])
        up = [(i, (i + 1) % count) for i in range(count - 1)]
        down = [(j, i) for i, j in up]
        last = lax.slice_in_dim(x, length - width, length, axis=dim)
        initial = lax.slice_in_dim(x, 0, width, axis=dim)
        before = lax.ppermute(last, axis, up)
        after = lax.ppermute(initial, axis, down)
        x = jnp.concatenate([before, x, after], axis=dim)
    return x


def modulate(rows_in, norm_gain, shift_vec, scale_vec):
    values = rows_in.astype(jnp.float32)
    normed = values * lax.rsqrt(jnp.mean(values * values, axis=-1, keepdims=True) + EPS)
    return (normed * norm_gain * (1.0 + scale_vec) + shift_vec).astype(jnp.bfloat16)


def head_norm(projected, head_gain):
    row_count = projected.shape[0]
    split_heads = projected.reshape(row_count, -1, head_gain.shape[0])
    normed = split_heads * lax.rsqrt(
        jnp.mean(split_heads * split_heads, axis=-1, keepdims=True) + EPS
    )
    return (normed * head_gain).astype(jnp.bfloat16).reshape(row_count, -1)


def per_device_plain(
    latent,
    context,
    condition,
    ctx_condition,
    shift_weight,
    scale_weight,
    gate_weight,
    norm_gain,
    query_weight,
    key_weight,
    value_weight,
    query_gain,
    key_gain,
    offset_bias,
    out_weight,
):
    activations = jax.nn.silu(jnp.stack([condition, ctx_condition])).astype(jnp.bfloat16)
    part_shift = jnp.dot(activations, shift_weight, preferred_element_type=jnp.float32)
    part_scale = jnp.dot(activations, scale_weight, preferred_element_type=jnp.float32)
    part_gate = jnp.dot(activations[:1], gate_weight, preferred_element_type=jnp.float32)
    block_cols = shift_weight.shape[1]
    first_col = lax.axis_index("tp") * block_cols

    def spread(piece_part):
        padded_vec = jnp.zeros((piece_part.shape[0], block_cols * lax.axis_size("tp")), jnp.float32)
        return lax.dynamic_update_slice_in_dim(padded_vec, piece_part, first_col, 1)

    shift_vec, scale_vec, gate_vec = lax.psum(
        (spread(part_shift), spread(part_scale), spread(part_gate)), ("sp", "tp")
    )
    hidden = modulate(latent, norm_gain, shift_vec[0], scale_vec[0])
    queries = head_norm(
        jnp.dot(hidden, query_weight, preferred_element_type=jnp.float32), query_gain
    )
    keys_lat = head_norm(jnp.dot(hidden, key_weight, preferred_element_type=jnp.float32), key_gain)
    values_lat = jnp.dot(hidden, value_weight, preferred_element_type=jnp.float32).astype(
        jnp.bfloat16
    )
    ctx_hidden = modulate(
        lax.all_gather(context, "sp", axis=0, tiled=True), norm_gain, shift_vec[1], scale_vec[1]
    )
    ctx_keys = head_norm(
        jnp.dot(ctx_hidden, key_weight, preferred_element_type=jnp.float32), key_gain
    )
    ctx_values = jnp.dot(ctx_hidden, value_weight, preferred_element_type=jnp.float32).astype(
        jnp.bfloat16
    )
    ctx_pairs = jnp.concatenate([ctx_keys, ctx_values], axis=1)
    col_width = keys_lat.shape[1]
    heads_dev = col_width // HEAD_DIM
    local_rows = keys_lat.shape[0] // GRID_W
    halo_rows = WIN_ROWS // 2
    window_keys = WIN_ROWS * GRID_W
    key_value = jnp.concatenate([keys_lat, values_lat], axis=1).reshape(
        local_rows, GRID_W, 2 * col_width
    )
    padded = extended(key_value, (("sp", 0),), halo_rows)
    first_row = lax.axis_index("sp") * local_rows
    total_rows = local_rows * lax.axis_size("sp")
    global_rows = first_row + jnp.arange(local_rows, dtype=jnp.int32)
    band_start = jnp.clip(global_rows - halo_rows, 0, total_rows - WIN_ROWS)
    band_global = band_start[:, None] + jnp.arange(WIN_ROWS, dtype=jnp.int32)[None, :]
    banded = jnp.take(padded, band_global - first_row + halo_rows, axis=0)
    key_band = banded[..., :col_width].reshape(local_rows, window_keys, heads_dev, HEAD_DIM)
    value_band = banded[..., col_width:].reshape(local_rows, window_keys, heads_dev, HEAD_DIM)
    row_steps = band_global - global_rows[:, None] + WIN_ROWS - 1
    row_hot = (
        row_steps[:, :, None] == jnp.arange(2 * WIN_ROWS - 1, dtype=jnp.int32)[None, None, :]
    ).astype(jnp.float32)
    column_ids = jnp.arange(GRID_W, dtype=jnp.int32)
    col_steps = (
        jnp.clip(column_ids[None, :] - column_ids[:, None], 1 - WIN_COLS, WIN_COLS - 1)
        + WIN_COLS
        - 1
    )
    col_hot = (
        col_steps[:, :, None] == jnp.arange(2 * WIN_COLS - 1, dtype=jnp.int32)[None, None, :]
    ).astype(jnp.float32)
    col_start = jnp.clip(column_ids - WIN_COLS // 2, 0, GRID_W - WIN_COLS)
    col_open = (column_ids[None, :] >= col_start[:, None]) & (
        column_ids[None, :] < col_start[:, None] + WIN_COLS
    )
    col_table = jnp.einsum("hab,qkb->haqk", offset_bias, col_hot, precision=lax.Precision.HIGHEST)
    col_table = jnp.where(col_open[None, None, :, :], col_table, -jnp.inf)
    offset_terms = jnp.einsum(
        "rja,haqk->hrqjk",
        row_hot,
        jnp.where(col_open[None, None], col_table, 0.0),
        precision=lax.Precision.HIGHEST,
    )
    offset_terms = jnp.where(col_open[None, None, :, None, :], offset_terms, -jnp.inf)
    offset_terms = offset_terms.reshape(heads_dev, local_rows, GRID_W, window_keys)
    score_scale = HEAD_DIM ** (-0.5)
    q_grid = queries.reshape(local_rows, GRID_W, heads_dev, HEAD_DIM)
    scores = (
        jnp.einsum("rqhd,rnhd->hrqn", q_grid, key_band, preferred_element_type=jnp.float32)
        * score_scale
        + offset_terms
    )
    ctx_count = ctx_pairs.shape[0]
    ctx_keys_all = ctx_pairs[:, :col_width].reshape(ctx_count, heads_dev, HEAD_DIM)
    ctx_values_all = ctx_pairs[:, col_width:].reshape(ctx_count, heads_dev, HEAD_DIM)
    ctx_scores = (
        jnp.einsum("rqhd,nhd->hrqn", q_grid, ctx_keys_all, preferred_element_type=jnp.float32)
        * score_scale
    )
    row_max = jnp.maximum(jnp.max(scores, axis=3), jnp.max(ctx_scores, axis=3))
    local_exp = jnp.exp(scores - row_max[..., None])
    ctx_exp = jnp.exp(ctx_scores - row_max[..., None])
    denominator = jnp.sum(local_exp, axis=3) + jnp.sum(ctx_exp, axis=3)
    local_weights = (local_exp / denominator[..., None]).astype(jnp.bfloat16)
    ctx_weights = (ctx_exp / denominator[..., None]).astype(jnp.bfloat16)
    combined = jnp.einsum(
        "hrqn,rnhd->rqhd", local_weights, value_band, preferred_element_type=jnp.float32
    ) + jnp.einsum(
        "hrqn,nhd->rqhd", ctx_weights, ctx_values_all, preferred_element_type=jnp.float32
    )
    attended = combined.astype(jnp.bfloat16).reshape(local_rows * GRID_W, col_width)
    partial_value = jnp.dot(attended, out_weight, preferred_element_type=jnp.float32)
    branch = lax.psum(partial_value.astype(jnp.bfloat16), "tp").astype(jnp.float32)
    return (latent.astype(jnp.float32) + gate_vec[0] * branch).astype(jnp.bfloat16)


MESH = pl.DeviceIdType.MESH
MASKED = -1e30
F32 = jnp.float32
BF16 = jnp.bfloat16


def fused_kernel(
    n_sp,
    n_tp,
    latent,
    context,
    shift_w,
    scale_w,
    gate_w,
    query_w,
    key_w,
    value_w,
    out_w,
    cond,
    ctx_cond,
    norm_gain,
    query_gain,
    key_gain,
    bias_in,
    out,
    x_in,
    x_norm,
    hid,
    w_mod,
    w_qkv,
    w_out,
    mod_sp,
    mod_tp,
    q_stage,
    k_stage,
    v_stage,
    ck_stage,
    cv_stage,
    q_all,
    k_all,
    v_all,
    ctx_k,
    ctx_v,
    bias_pad,
    bias_lines,
    table,
    att_slab,
    att,
    local_sem,
    mod_send,
    mod_recv,
    modt_send,
    modt_recv,
    pair_send,
    pair_recv,
    halo_send,
    halo_recv,
    ctx_send,
    ctx_recv,
    wo_send,
    wo_recv,
    att_send,
    att_recv,
):
    me_s, me_t = lax.axis_index("sp"), lax.axis_index("tp")
    rows, d = latent.shape
    c_rows = context.shape[0]
    width = key_w.shape[1]
    heads = width // HEAD_DIM
    block = shift_w.shape[1]
    l_rows = rows // GRID_W
    halo = WIN_ROWS // 2
    win = WIN_ROWS * GRID_W
    core = lax.rem(me_t, 2)
    chip = lax.div(me_t, 2)
    partner = me_t + 1 - 2 * core
    n_x = n_tp // 2
    side = lax.rem(me_s, 2)
    slab = lax.div(me_s, 2)
    mate = me_s + 1 - 2 * side
    last_slab = n_sp // 2 - 1
    half = width // 2
    half_heads = heads // 2

    def remote(src, dst, send, recv, s, t):
        return pltpu.make_async_remote_copy(
            src_ref=src, dst_ref=dst, send_sem=send, recv_sem=recv,
            device_id=(s, t), device_id_type=MESH,
        )

    barrier = pltpu.get_barrier_semaphore()
    for k in range(1, n_sp):
        pl.semaphore_signal(
            barrier, inc=1, device_id=(lax.rem(me_s + k, n_sp), me_t), device_id_type=MESH
        )
    for k in range(1, n_tp):
        pl.semaphore_signal(
            barrier, inc=1, device_id=(me_s, lax.rem(me_t + k, n_tp)), device_id_type=MESH
        )

    loads = [
        (shift_w, w_mod.at[0]),
        (scale_w, w_mod.at[1]),
        (gate_w, w_mod.at[2]),
        (context, x_in.at[pl.ds(0, c_rows)]),
        (latent, x_in.at[pl.ds(c_rows, rows)]),
        (key_w, w_qkv.at[0]),
        (value_w, w_qkv.at[1]),
        (query_w, w_qkv.at[2]),
        (out_w, w_out.at[me_t]),
    ]
    copies = [pltpu.make_async_copy(a, b, local_sem.at[i]) for i, (a, b) in enumerate(loads)]
    for c in copies:
        c.start()

    def silu(v):
        return v / (1.0 + jnp.exp(-v))

    two = (16, cond.shape[1])
    row_id = lax.broadcasted_iota(jnp.int32, two, 0)
    act0 = jnp.broadcast_to(silu(cond[...]), two)
    act1 = jnp.broadcast_to(silu(ctx_cond[...]), two)

    def placed(first, second):
        picked = jnp.where(row_id == first, act0, 0.0)
        if second is not None:
            picked = jnp.where(row_id == second, act1, picked)
        return picked.astype(BF16)

    part = jnp.zeros((16, block), F32)
    for i, (first, second) in enumerate(((0, 1), (2, 3), (4, None))):
        copies[i].wait()
        part += jnp.dot(placed(first, second), w_mod[i], preferred_element_type=F32)
    mod_sp[me_s] = part[:8]
    pl.semaphore_wait(barrier, n_sp + n_tp - 2)
    sends = []
    for k in range(1, n_sp):
        peer = lax.rem(me_s + k, n_sp)
        c = remote(
            mod_sp.at[me_s], mod_sp.at[me_s], mod_send.at[k], mod_recv.at[me_s], peer, me_t
        )
        c.start()
        sends.append(c)

    copies[3].wait()
    copies[4].wait()
    step = 32

    def norm_rows(i, carry):
        at = pl.ds(pl.multiple_of(i * step, step), step)
        v = x_in[at, :].astype(F32)
        r = lax.rsqrt(jnp.mean(v * v, axis=-1, keepdims=True) + EPS)
        x_norm[at, :] = v * r * norm_gain[...]
        return carry

    lax.fori_loop(0, (rows + c_rows) // step, norm_rows, 0)

    pair = 2 * GRID_W
    q_col = lax.broadcasted_iota(jnp.int32, (GRID_W, pair), 0)
    k_col = lax.broadcasted_iota(jnp.int32, (GRID_W, pair), 1) % GRID_W
    col0 = jnp.clip(q_col - WIN_COLS // 2, 0, GRID_W - WIN_COLS)
    col_open = (k_col >= col0) & (k_col < col0 + WIN_COLS)
    n_pairs = 2 * WIN_ROWS - 2
    bias_pad[...] = jnp.zeros_like(bias_pad)
    for h in range(heads):
        bias_pad[h, : 2 * WIN_ROWS - 1, : 2 * WIN_COLS - 1] = bias_in[h]
    for h in range(half_heads):
        head = side * half_heads + h
        upper = pltpu.roll(bias_pad[head, 1 : n_pairs + 1, :], GRID_W, 1)
        bias_lines[h, :n_pairs, :] = bias_pad[head, :n_pairs, :] + upper
        for a in range(n_pairs):
            line = jnp.broadcast_to(bias_lines[h, a : a + 1, :], (GRID_W, pair))
            rolled = pltpu.roll(line, pair - (WIN_COLS - 1), 1, stride=1, stride_axis=0)
            table[a, h * GRID_W : (h + 1) * GRID_W, :] = jnp.where(col_open, rolled, MASKED)

    for k in range(1, n_sp):
        peer = lax.rem(me_s + k, n_sp)
        remote(
            mod_sp.at[peer], mod_sp.at[peer], mod_send.at[k], mod_recv.at[peer], peer, me_t
        ).wait_recv()
    total = mod_sp[0]
    for k in range(1, n_sp):
        total = total + mod_sp[k]
    mod_tp[me_t] = total
    for k in range(1, n_tp):
        peer = lax.rem(me_t + k, n_tp)
        c = remote(
            mod_tp.at[me_t], mod_tp.at[me_t], modt_send.at[k], modt_recv.at[me_t], me_s, peer
        )
        c.start()
        sends.append(c)

    def gather_start(buf, send, recv):
        started = [remote(buf.at[me_t], buf.at[me_t], send.at[0], recv.at[me_t], me_s, partner)]
        for k in range(1, n_x):
            far = 2 * lax.rem(chip + k, n_x) + core
            started.append(
                remote(buf.at[me_t], buf.at[me_t], send.at[k], recv.at[me_t], me_s, far)
            )
        for c in reversed(started):
            c.start()
        sends.extend(started)

    def gather_forward(buf, send, recv):
        for k in range(1, n_x):
            came = 2 * lax.rem(chip + n_x - k, n_x) + core
            c = remote(
                buf.at[came], buf.at[came], send.at[n_x + k], recv.at[came], me_s, partner
            )
            c.wait_recv()
            c.start()
            sends.append(c)

    def gather_finish(buf, send, recv):
        remote(
            buf.at[partner], buf.at[partner], send.at[0], recv.at[partner], me_s, partner
        ).wait_recv()
        for k in range(1, n_x):
            came = 2 * lax.rem(chip + n_x - k, n_x) + 1 - core
            remote(
                buf.at[came], buf.at[came], send.at[n_x + k], recv.at[came], me_s, partner
            ).wait_recv()

    for k in range(1, n_tp):
        peer = lax.rem(me_t + k, n_tp)
        remote(
            mod_tp.at[peer], mod_tp.at[peer], modt_send.at[k], modt_recv.at[peer], me_s, peer
        ).wait_recv()
    copies[8].wait()
    gather_start(w_out, wo_send, wo_recv)

    def vec(r):
        return jnp.concatenate([mod_tp[j][r : r + 1, :] for j in range(n_tp)], axis=1)

    def modulate_rows(first, count, shift, scale):
        def body(i, carry):
            at = pl.ds(pl.multiple_of(first + i * step, step), step)
            hid[at, :] = (x_norm[at, :] * scale + shift).astype(BF16)
            return carry

        lax.fori_loop(0, count // step, body, 0)

    modulate_rows(0, c_rows, vec(1), 1.0 + vec(3))
    modulate_rows(c_rows, rows, vec(0), 1.0 + vec(2))

    head_row = lax.broadcasted_iota(jnp.int32, (width, width), 0) // HEAD_DIM
    head_col = lax.broadcasted_iota(jnp.int32, (width, width), 1) // HEAD_DIM
    same_head = (head_row == head_col).astype(F32)

    def head_scale(p, gain):
        mean = jnp.dot(
            p * p, same_head, precision=lax.Precision.HIGHEST, preferred_element_type=F32
        ) * (1.0 / HEAD_DIM)
        wide_gain = jnp.concatenate([gain[...]] * heads, axis=1)
        return (p * lax.rsqrt(mean + EPS) * wide_gain).astype(BF16)

    own = pl.ds(rows + pl.multiple_of(side * rows, rows), rows)
    other = pl.ds(rows + pl.multiple_of((1 - side) * rows, rows), rows)

    def split(stage, value):
        for h in range(2):
            stage[h] = value[:, h * half : (h + 1) * half]

    def trade(index, stage, block_all, at):
        c = remote(
            stage.at[1 - side], block_all.at[at], pair_send.at[index], pair_recv.at[index],
            mate, me_t,
        )
        c.start()
        sends.append(c)
        return c

    def share_ctx(index, stage, block_ctx):
        block_ctx[me_s] = stage[side]
        for k in range(1, n_sp):
            peer = lax.rem(me_s + k, n_sp)
            c = remote(
                stage.at[lax.rem(peer, 2)], block_ctx.at[me_s],
                ctx_send.at[index, k], ctx_recv.at[index, me_s], peer, me_t,
            )
            c.start()
            sends.append(c)

    def halo_copies(index, block_all):
        down = remote(
            block_all.at[pl.ds(rows, rows)], block_all.at[pl.ds(3 * rows, rows)],
            halo_send.at[index, 0], halo_recv.at[index, 0], me_s - 2, me_t,
        )
        up = remote(
            block_all.at[pl.ds(2 * rows, rows)], block_all.at[pl.ds(0, rows)],
            halo_send.at[index, 1], halo_recv.at[index, 1], me_s + 2, me_t,
        )
        return down, up

    def halo_start(mine):
        for index, block_all in enumerate((k_all, v_all)):
            down, up = halo_copies(index, block_all)
            is_low = side == 0 if mine else side == 1

            @pl.when(is_low & (slab > 0))
            def _():
                down.start()

            @pl.when(jnp.logical_not(is_low) & (slab < last_slab))
            def _():
                up.start()

    copies[5].wait()
    keys = head_scale(jnp.dot(hid[...], w_qkv[0], preferred_element_type=F32), key_gain)
    split(k_stage, keys[c_rows:])
    k_trade = trade(0, k_stage, k_all, own)
    split(ck_stage, keys[:c_rows])
    k_all[own, :] = k_stage[side]
    copies[6].wait()
    values = jnp.dot(hid[...], w_qkv[1], preferred_element_type=F32).astype(BF16)
    split(v_stage, values[c_rows:])
    v_trade = trade(1, v_stage, v_all, own)
    split(cv_stage, values[:c_rows])
    v_all[own, :] = v_stage[side]
    halo_start(True)
    share_ctx(0, ck_stage, ctx_k)
    share_ctx(1, cv_stage, ctx_v)
    copies[7].wait()
    queries = head_scale(
        jnp.dot(hid[c_rows:, :], w_qkv[2], preferred_element_type=F32), query_gain
    ) * jnp.asarray(HEAD_DIM ** (-0.5), BF16)
    split(q_stage, queries)
    q_own = pl.ds(pl.multiple_of(side * rows, rows), rows)
    q_trade = trade(2, q_stage, q_all, q_own)
    q_all[q_own, :] = q_stage[side]
    k_trade.wait_recv()
    v_trade.wait_recv()
    halo_start(False)
    q_trade.wait_recv()

    for index, block_ctx in enumerate((ctx_k, ctx_v)):
        for k in range(1, n_sp):
            peer = lax.rem(me_s + k, n_sp)
            remote(
                block_ctx.at[peer], block_ctx.at[peer],
                ctx_send.at[index, k], ctx_recv.at[index, peer], peer, me_t,
            ).wait_recv()
    for index, block_all in enumerate((k_all, v_all)):
        down, up = halo_copies(index, block_all)

        @pl.when(slab < last_slab)
        def _():
            down.wait_recv()

        @pl.when(slab > 0)
        def _():
            up.wait_recv()

    lane_head = lax.broadcasted_iota(jnp.int32, (GRID_W, half), 1) // HEAD_DIM
    masks = [(lane_head == h).astype(F32) for h in range(half_heads)]
    contract_last = (((1,), (1,)), ((), ()))
    all_ck = ctx_k[...].reshape(n_sp * c_rows, half)
    all_cv = ctx_v[...].reshape(n_sp * c_rows, half)

    def attend(i):
        start = jnp.where(
            slab == 0,
            jnp.maximum(i, halo),
            jnp.where(slab == last_slab, jnp.minimum(i, halo), i),
        )
        if last_slab == 0:
            start = jnp.int32(halo)
        at = pl.ds(pl.multiple_of(start * GRID_W, GRID_W), win)
        row_at = pl.ds(pl.multiple_of(i * GRID_W, GRID_W), GRID_W)
        qi = q_all[row_at, :].astype(F32)
        qs = jnp.concatenate([(qi * m).astype(BF16) for m in masks], axis=0)
        s1 = lax.dot_general(qs, k_all[at, :], contract_last, preferred_element_type=F32)
        first = start - i + WIN_ROWS - 1 - halo
        s1 = s1 + jnp.concatenate([table[first + 2 * m] for m in range(WIN_ROWS // 2)], axis=1)
        s2 = lax.dot_general(qs, all_ck, contract_last, preferred_element_type=F32)
        top = jnp.maximum(
            jnp.max(s1, axis=1, keepdims=True), jnp.max(s2, axis=1, keepdims=True)
        )
        e1 = jnp.exp(s1 - top)
        e2 = jnp.exp(s2 - top)
        inv = 1.0 / (jnp.sum(e1, axis=1, keepdims=True) + jnp.sum(e2, axis=1, keepdims=True))
        o = jnp.dot((e1 * inv).astype(BF16), v_all[at, :], preferred_element_type=F32)
        o = o + jnp.dot((e2 * inv).astype(BF16), all_cv, preferred_element_type=F32)
        picked = o[:GRID_W] * masks[0]
        for h in range(1, half_heads):
            picked = picked + o[h * GRID_W : (h + 1) * GRID_W] * masks[h]
        return picked.astype(BF16)

    for i in range(l_rows):
        att_slab[i * GRID_W : (i + 1) * GRID_W, :] = attend((1 - side) * l_rows + i)
    back = remote(
        att_slab, att.at[me_t, side], pair_send.at[3], pair_recv.at[3], mate, me_t
    )
    back.start()
    sends.append(back)
    for i in range(l_rows):
        att[me_t, side, i * GRID_W : (i + 1) * GRID_W, :] = attend(side * l_rows + i)

    back_in = remote(
        att_slab, att.at[me_t, 1 - side], pair_send.at[3], pair_recv.at[3], mate, me_t
    )
    back_in.wait_recv()
    gather_forward(w_out, wo_send, wo_recv)
    gather_start(att, att_send, att_recv)
    gather_forward(att, att_send, att_recv)
    gather_finish(w_out, wo_send, wo_recv)
    gather_finish(att, att_send, att_recv)
    gate = vec(4)
    cols = 512
    for n in range(d // cols):
        at = slice(n * cols, (n + 1) * cols)
        branch = jnp.zeros((rows, cols), F32)
        for j in range(n_tp):
            branch = branch + jnp.dot(
                jnp.concatenate([att[j, 0], att[j, 1]], axis=1),
                w_out[j, :, at],
                preferred_element_type=F32,
            ).astype(BF16).astype(F32)
        base = x_in[c_rows:, at].astype(F32)
        out[:, at] = (base + gate[:, at] * branch).astype(BF16)

    for c in sends:
        c.wait_send()
    for index, block_all in enumerate((k_all, v_all)):
        down, up = halo_copies(index, block_all)

        @pl.when(slab > 0)
        def _():
            down.wait_send()

        @pl.when(slab < last_slab)
        def _():
            up.wait_send()


def per_device(
    latent,
    context,
    condition,
    ctx_condition,
    shift_weight,
    scale_weight,
    gate_weight,
    norm_gain,
    query_weight,
    key_weight,
    value_weight,
    query_gain,
    key_gain,
    offset_bias,
    out_weight,
):
    n_sp, n_tp = lax.axis_size("sp"), lax.axis_size("tp")
    rows, d = latent.shape
    c_rows = context.shape[0]
    width = key_weight.shape[1]
    heads = width // HEAD_DIM
    block = shift_weight.shape[1]
    n_pairs = 2 * WIN_ROWS - 2
    half = width // 2
    half_heads = heads // 2
    any_spec = pl.BlockSpec(memory_space=pl.ANY)
    vmem_spec = pl.BlockSpec(memory_space=pltpu.VMEM)
    dma = pltpu.SemaphoreType.DMA
    return pl.pallas_call(
        functools.partial(fused_kernel, n_sp, n_tp),
        out_shape=jax.ShapeDtypeStruct((rows, d), BF16),
        in_specs=[any_spec] * 9 + [vmem_spec] * 6,
        out_specs=vmem_spec,
        scratch_shapes=[
            pltpu.VMEM((rows + c_rows, d), BF16),
            pltpu.VMEM((rows + c_rows, d), F32),
            pltpu.VMEM((rows + c_rows, d), BF16),
            pltpu.VMEM((3, shift_weight.shape[0], block), BF16),
            pltpu.VMEM((3, d, width), BF16),
            pltpu.VMEM((n_tp, width, d), BF16),
            pltpu.VMEM((n_sp, 8, block), F32),
            pltpu.VMEM((n_tp, 8, block), F32),
            pltpu.VMEM((2, rows, half), BF16),
            pltpu.VMEM((2, rows, half), BF16),
            pltpu.VMEM((2, rows, half), BF16),
            pltpu.VMEM((2, c_rows, half), BF16),
            pltpu.VMEM((2, c_rows, half), BF16),
            pltpu.VMEM((2 * rows, half), BF16),
            pltpu.VMEM((4 * rows, half), BF16),
            pltpu.VMEM((4 * rows, half), BF16),
            pltpu.VMEM((n_sp, c_rows, half), BF16),
            pltpu.VMEM((n_sp, c_rows, half), BF16),
            pltpu.VMEM((heads, 2 * WIN_ROWS, 2 * GRID_W), F32),
            pltpu.VMEM((half_heads, 2 * WIN_ROWS, 2 * GRID_W), F32),
            pltpu.VMEM((n_pairs, half_heads * GRID_W, 2 * GRID_W), F32),
            pltpu.VMEM((rows, half), BF16),
            pltpu.VMEM((n_tp, 2, rows, half), BF16),
            dma((9,)),
            dma((n_sp,)),
            dma((n_sp,)),
            dma((n_tp,)),
            dma((n_tp,)),
            dma((4,)),
            dma((4,)),
            dma((2, 2)),
            dma((2, 2)),
            dma((2, n_sp)),
            dma((2, n_sp)),
            dma((n_tp,)),
            dma((n_tp,)),
            dma((n_tp,)),
            dma((n_tp,)),
        ],
        compiler_params=pltpu.CompilerParams(collective_id=0, has_side_effects=True),
        name="fused_block",
    )(
        latent,
        context,
        shift_weight,
        scale_weight,
        gate_weight,
        query_weight,
        key_weight,
        value_weight,
        out_weight,
        condition.reshape(1, -1),
        ctx_condition.reshape(1, -1),
        norm_gain.reshape(1, -1),
        query_gain.reshape(1, -1),
        key_gain.reshape(1, -1),
        offset_bias,
    )


def fused_fits(latent, context, condition, query_weight, n_sp, n_tp):
    rows, c_rows = latent.shape[0] // n_sp, context.shape[0] // n_sp
    width = query_weight.shape[1] // n_tp
    return (
        rows == WIN_ROWS // 2 * GRID_W
        and c_rows % 32 == 0
        and condition.shape[0] // n_sp % 128 == 0
        and width % 256 == 0
        and n_tp % 2 == 0
        and n_sp % 2 == 0
    )


def solution(mesh):
    in_specs = (
        P("sp", None),
        P("sp", None),
        P("sp"),
        P("sp"),
        P("sp", "tp"),
        P("sp", "tp"),
        P("sp", "tp"),
        P(),
        P(None, "tp"),
        P(None, "tp"),
        P(None, "tp"),
        P(),
        P(),
        P("tp", None, None),
        P("tp", None),
    )
    out_specs = P("sp", None)

    def step(latent, context, condition, ctx_condition, *rest):
        n_sp, n_tp = mesh.shape["sp"], mesh.shape["tp"]
        fits = fused_fits(latent, context, condition, rest[4], n_sp, n_tp)
        body = per_device if fits else per_device_plain
        return jax.shard_map(
            body, mesh=mesh, in_specs=in_specs, out_specs=out_specs, check_vma=False
        )(latent, context, condition, ctx_condition, *rest)

    return step
```

```python
import functools

import jax
import jax.numpy as jnp
from jax import lax
from jax.experimental import pallas as pl
from jax.experimental.pallas import tpu as pltpu
from jax.sharding import PartitionSpec as P

HEAD_DIM = 64
GRID_W = 64
WIN_ROWS = 8
WIN_COLS = 16


EPS = 1e-06


def extended(x, sides, width):
    for axis, dim in sides:
        count, length = (lax.axis_size(axis), x.shape[dim])
        up = [(i, (i + 1) % count) for i in range(count - 1)]
        down = [(j, i) for i, j in up]
        last = lax.slice_in_dim(x, length - width, length, axis=dim)
        initial = lax.slice_in_dim(x, 0, width, axis=dim)
        before = lax.ppermute(last, axis, up)
        after = lax.ppermute(initial, axis, down)
        x = jnp.concatenate([before, x, after], axis=dim)
    return x


def modulate(rows_in, norm_gain, shift_vec, scale_vec):
    values = rows_in.astype(jnp.float32)
    normed = values * lax.rsqrt(jnp.mean(values * values, axis=-1, keepdims=True) + EPS)
    return (normed * norm_gain * (1.0 + scale_vec) + shift_vec).astype(jnp.bfloat16)


def head_norm(projected, head_gain):
    row_count = projected.shape[0]
    split_heads = projected.reshape(row_count, -1, head_gain.shape[0])
    normed = split_heads * lax.rsqrt(
        jnp.mean(split_heads * split_heads, axis=-1, keepdims=True) + EPS
    )
    return (normed * head_gain).astype(jnp.bfloat16).reshape(row_count, -1)


def per_device_plain(
    latent,
    context,
    condition,
    ctx_condition,
    shift_weight,
    scale_weight,
    gate_weight,
    norm_gain,
    query_weight,
    key_weight,
    value_weight,
    query_gain,
    key_gain,
    offset_bias,
    out_weight,
):
    activations = jax.nn.silu(jnp.stack([condition, ctx_condition])).astype(jnp.bfloat16)
    part_shift = jnp.dot(activations, shift_weight, preferred_element_type=jnp.float32)
    part_scale = jnp.dot(activations, scale_weight, preferred_element_type=jnp.float32)
    part_gate = jnp.dot(activations[:1], gate_weight, preferred_element_type=jnp.float32)
    block_cols = shift_weight.shape[1]
    first_col = lax.axis_index("tp") * block_cols

    def spread(piece_part):
        padded_vec = jnp.zeros((piece_part.shape[0], block_cols * lax.axis_size("tp")), jnp.float32)
        return lax.dynamic_update_slice_in_dim(padded_vec, piece_part, first_col, 1)

    shift_vec, scale_vec, gate_vec = lax.psum(
        (spread(part_shift), spread(part_scale), spread(part_gate)), ("sp", "tp")
    )
    hidden = modulate(latent, norm_gain, shift_vec[0], scale_vec[0])
    queries = head_norm(
        jnp.dot(hidden, query_weight, preferred_element_type=jnp.float32), query_gain
    )
    keys_lat = head_norm(jnp.dot(hidden, key_weight, preferred_element_type=jnp.float32), key_gain)
    values_lat = jnp.dot(hidden, value_weight, preferred_element_type=jnp.float32).astype(
        jnp.bfloat16
    )
    ctx_hidden = modulate(
        lax.all_gather(context, "sp", axis=0, tiled=True), norm_gain, shift_vec[1], scale_vec[1]
    )
    ctx_keys = head_norm(
        jnp.dot(ctx_hidden, key_weight, preferred_element_type=jnp.float32), key_gain
    )
    ctx_values = jnp.dot(ctx_hidden, value_weight, preferred_element_type=jnp.float32).astype(
        jnp.bfloat16
    )
    ctx_pairs = jnp.concatenate([ctx_keys, ctx_values], axis=1)
    col_width = keys_lat.shape[1]
    heads_dev = col_width // HEAD_DIM
    local_rows = keys_lat.shape[0] // GRID_W
    halo_rows = WIN_ROWS // 2
    window_keys = WIN_ROWS * GRID_W
    key_value = jnp.concatenate([keys_lat, values_lat], axis=1).reshape(
        local_rows, GRID_W, 2 * col_width
    )
    padded = extended(key_value, (("sp", 0),), halo_rows)
    first_row = lax.axis_index("sp") * local_rows
    total_rows = local_rows * lax.axis_size("sp")
    global_rows = first_row + jnp.arange(local_rows, dtype=jnp.int32)
    band_start = jnp.clip(global_rows - halo_rows, 0, total_rows - WIN_ROWS)
    band_global = band_start[:, None] + jnp.arange(WIN_ROWS, dtype=jnp.int32)[None, :]
    banded = jnp.take(padded, band_global - first_row + halo_rows, axis=0)
    key_band = banded[..., :col_width].reshape(local_rows, window_keys, heads_dev, HEAD_DIM)
    value_band = banded[..., col_width:].reshape(local_rows, window_keys, heads_dev, HEAD_DIM)
    row_steps = band_global - global_rows[:, None] + WIN_ROWS - 1
    row_hot = (
        row_steps[:, :, None] == jnp.arange(2 * WIN_ROWS - 1, dtype=jnp.int32)[None, None, :]
    ).astype(jnp.float32)
    column_ids = jnp.arange(GRID_W, dtype=jnp.int32)
    col_steps = (
        jnp.clip(column_ids[None, :] - column_ids[:, None], 1 - WIN_COLS, WIN_COLS - 1)
        + WIN_COLS
        - 1
    )
    col_hot = (
        col_steps[:, :, None] == jnp.arange(2 * WIN_COLS - 1, dtype=jnp.int32)[None, None, :]
    ).astype(jnp.float32)
    col_start = jnp.clip(column_ids - WIN_COLS // 2, 0, GRID_W - WIN_COLS)
    col_open = (column_ids[None, :] >= col_start[:, None]) & (
        column_ids[None, :] < col_start[:, None] + WIN_COLS
    )
    col_table = jnp.einsum("hab,qkb->haqk", offset_bias, col_hot, precision=lax.Precision.HIGHEST)
    col_table = jnp.where(col_open[None, None, :, :], col_table, -jnp.inf)
    offset_terms = jnp.einsum(
        "rja,haqk->hrqjk",
        row_hot,
        jnp.where(col_open[None, None], col_table, 0.0),
        precision=lax.Precision.HIGHEST,
    )
    offset_terms = jnp.where(col_open[None, None, :, None, :], offset_terms, -jnp.inf)
    offset_terms = offset_terms.reshape(heads_dev, local_rows, GRID_W, window_keys)
    score_scale = HEAD_DIM ** (-0.5)
    q_grid = queries.reshape(local_rows, GRID_W, heads_dev, HEAD_DIM)
    scores = (
        jnp.einsum("rqhd,rnhd->hrqn", q_grid, key_band, preferred_element_type=jnp.float32)
        * score_scale
        + offset_terms
    )
    ctx_count = ctx_pairs.shape[0]
    ctx_keys_all = ctx_pairs[:, :col_width].reshape(ctx_count, heads_dev, HEAD_DIM)
    ctx_values_all = ctx_pairs[:, col_width:].reshape(ctx_count, heads_dev, HEAD_DIM)
    ctx_scores = (
        jnp.einsum("rqhd,nhd->hrqn", q_grid, ctx_keys_all, preferred_element_type=jnp.float32)
        * score_scale
    )
    row_max = jnp.maximum(jnp.max(scores, axis=3), jnp.max(ctx_scores, axis=3))
    local_exp = jnp.exp(scores - row_max[..., None])
    ctx_exp = jnp.exp(ctx_scores - row_max[..., None])
    denominator = jnp.sum(local_exp, axis=3) + jnp.sum(ctx_exp, axis=3)
    local_weights = (local_exp / denominator[..., None]).astype(jnp.bfloat16)
    ctx_weights = (ctx_exp / denominator[..., None]).astype(jnp.bfloat16)
    combined = jnp.einsum(
        "hrqn,rnhd->rqhd", local_weights, value_band, preferred_element_type=jnp.float32
    ) + jnp.einsum(
        "hrqn,nhd->rqhd", ctx_weights, ctx_values_all, preferred_element_type=jnp.float32
    )
    attended = combined.astype(jnp.bfloat16).reshape(local_rows * GRID_W, col_width)
    partial_value = jnp.dot(attended, out_weight, preferred_element_type=jnp.float32)
    branch = lax.psum(partial_value.astype(jnp.bfloat16), "tp").astype(jnp.float32)
    return (latent.astype(jnp.float32) + gate_vec[0] * branch).astype(jnp.bfloat16)


MESH = pl.DeviceIdType.MESH
MASKED = -1e30
F32 = jnp.float32
BF16 = jnp.bfloat16


def fused_kernel(
    n_sp,
    n_tp,
    latent,
    context,
    shift_w,
    scale_w,
    gate_w,
    query_w,
    key_w,
    value_w,
    out_w,
    cond,
    ctx_cond,
    norm_gain,
    query_gain,
    key_gain,
    bias_in,
    out,
    x_in,
    x_norm,
    hid,
    w_mod,
    w_qkv,
    w_out,
    mod_sp,
    mod_tp,
    q_stage,
    k_stage,
    v_stage,
    ck_stage,
    cv_stage,
    q_all,
    k_all,
    v_all,
    ctx_k,
    ctx_v,
    bias_pad,
    bias_lines,
    table,
    att_slab,
    att,
    local_sem,
    mod_send,
    mod_recv,
    modt_send,
    modt_recv,
    pair_send,
    pair_recv,
    halo_send,
    halo_recv,
    ctx_send,
    ctx_recv,
    wo_send,
    wo_recv,
    att_send,
    att_recv,
):
    me_s, me_t = lax.axis_index("sp"), lax.axis_index("tp")
    rows, d = latent.shape
    c_rows = context.shape[0]
    width = key_w.shape[1]
    heads = width // HEAD_DIM
    block = shift_w.shape[1]
    l_rows = rows // GRID_W
    halo = WIN_ROWS // 2
    win = WIN_ROWS * GRID_W
    core = lax.rem(me_t, 2)
    chip = lax.div(me_t, 2)
    partner = me_t + 1 - 2 * core
    n_x = n_tp // 2
    side = lax.rem(me_s, 2)
    slab = lax.div(me_s, 2)
    mate = me_s + 1 - 2 * side
    last_slab = n_sp // 2 - 1
    half = width // 2
    half_heads = heads // 2

    def remote(src, dst, send, recv, s, t):
        return pltpu.make_async_remote_copy(
            src_ref=src, dst_ref=dst, send_sem=send, recv_sem=recv,
            device_id=(s, t), device_id_type=MESH,
        )

    barrier = pltpu.get_barrier_semaphore()
    for k in range(1, n_sp):
        pl.semaphore_signal(
            barrier, inc=1, device_id=(lax.rem(me_s + k, n_sp), me_t), device_id_type=MESH
        )
    for k in range(1, n_tp):
        pl.semaphore_signal(
            barrier, inc=1, device_id=(me_s, lax.rem(me_t + k, n_tp)), device_id_type=MESH
        )

    loads = [
        (shift_w, w_mod.at[0]),
        (scale_w, w_mod.at[1]),
        (gate_w, w_mod.at[2]),
        (context, x_in.at[pl.ds(0, c_rows)]),
        (latent, x_in.at[pl.ds(c_rows, rows)]),
        (key_w, w_qkv.at[0]),
        (value_w, w_qkv.at[1]),
        (query_w, w_qkv.at[2]),
        (out_w, w_out.at[me_t]),
    ]
    copies = [pltpu.make_async_copy(a, b, local_sem.at[i]) for i, (a, b) in enumerate(loads)]
    for c in copies[:3]:
        c.start()

    def silu(v):
        return v / (1.0 + jnp.exp(-v))

    two = (16, cond.shape[1])
    row_id = lax.broadcasted_iota(jnp.int32, two, 0)
    act0 = jnp.broadcast_to(silu(cond[...]), two)
    act1 = jnp.broadcast_to(silu(ctx_cond[...]), two)

    def placed(first, second):
        picked = jnp.where(row_id == first, act0, 0.0)
        if second is not None:
            picked = jnp.where(row_id == second, act1, picked)
        return picked.astype(BF16)

    part = jnp.zeros((16, block), F32)
    for i, (first, second) in enumerate(((0, 1), (2, 3), (4, None))):
        copies[i].wait()
        part += jnp.dot(placed(first, second), w_mod[i], preferred_element_type=F32)
    for c in copies[3:]:
        c.start()
    mod_sp[me_s] = part[:8]
    pl.semaphore_wait(barrier, n_sp + n_tp - 2)
    sends = []
    for k in range(1, n_sp):
        peer = lax.rem(me_s + k, n_sp)
        c = remote(
            mod_sp.at[me_s], mod_sp.at[me_s], mod_send.at[k], mod_recv.at[me_s], peer, me_t
        )
        c.start()
        sends.append(c)

    def gather_start(view, sems, source=None):
        send, recv = sems
        mine = view(me_t) if source is None else source
        started = [remote(mine, view(me_t), send(0), recv(me_t), me_s, partner)]
        for k in range(1, n_x):
            far = 2 * lax.rem(chip + k, n_x) + core
            started.append(remote(mine, view(me_t), send(k), recv(me_t), me_s, far))
        for c in reversed(started):
            c.start()
        sends.extend(started)

    def gather_forward(view, sems):
        send, recv = sems
        for k in range(1, n_x):
            came = 2 * lax.rem(chip + n_x - k, n_x) + core
            c = remote(view(came), view(came), send(n_x + k), recv(came), me_s, partner)
            c.wait_recv()
            c.start()
            sends.append(c)

    def gather_finish(view, sems):
        send, recv = sems
        remote(
            view(partner), view(partner), send(0), recv(partner), me_s, partner
        ).wait_recv()
        for k in range(1, n_x):
            came = 2 * lax.rem(chip + n_x - k, n_x) + 1 - core
            remote(
                view(came), view(came), send(n_x + k), recv(came), me_s, partner
            ).wait_recv()

    early = width // 4
    wo_rows = (pl.ds(0, early), pl.ds(early, width - early))

    def wo_view(c):
        return lambda j: w_out.at[j, wo_rows[c]]

    def wo_source(c):
        return out_w.at[wo_rows[c]]

    def wo_sems(c):
        return (lambda k: wo_send.at[c, k]), (lambda k: wo_recv.at[c, k])

    def att_view(h):
        return lambda j: att.at[j, h]

    def att_sems(n):
        return (lambda k: att_send.at[n, k]), (lambda k: att_recv.at[n, k])

    gather_start(wo_view(0), wo_sems(0), wo_source(0))

    copies[3].wait()
    copies[4].wait()
    step = 32

    def norm_rows(i, carry):
        at = pl.ds(pl.multiple_of(i * step, step), step)
        v = x_in[at, :].astype(F32)
        r = lax.rsqrt(jnp.mean(v * v, axis=-1, keepdims=True) + EPS)
        x_norm[at, :] = v * r * norm_gain[...]
        return carry

    lax.fori_loop(0, (rows + c_rows) // step, norm_rows, 0)

    pair = 2 * GRID_W
    q_col = lax.broadcasted_iota(jnp.int32, (GRID_W, pair), 0)
    k_col = lax.broadcasted_iota(jnp.int32, (GRID_W, pair), 1) % GRID_W
    col0 = jnp.clip(q_col - WIN_COLS // 2, 0, GRID_W - WIN_COLS)
    col_open = (k_col >= col0) & (k_col < col0 + WIN_COLS)
    n_pairs = 2 * WIN_ROWS - 2
    bias_pad[...] = jnp.zeros_like(bias_pad)
    for h in range(heads):
        bias_pad[h, : 2 * WIN_ROWS - 1, : 2 * WIN_COLS - 1] = bias_in[h]
    for h in range(half_heads):
        head = side * half_heads + h
        upper = pltpu.roll(bias_pad[head, 1 : n_pairs + 1, :], GRID_W, 1)
        bias_lines[h, :n_pairs, :] = bias_pad[head, :n_pairs, :] + upper
        for a in range(n_pairs):
            line = jnp.broadcast_to(bias_lines[h, a : a + 1, :], (GRID_W, pair))
            rolled = pltpu.roll(line, pair - (WIN_COLS - 1), 1, stride=1, stride_axis=0)
            table[a, h * GRID_W : (h + 1) * GRID_W, :] = jnp.where(col_open, rolled, MASKED)

    for k in range(1, n_sp):
        peer = lax.rem(me_s + k, n_sp)
        remote(
            mod_sp.at[peer], mod_sp.at[peer], mod_send.at[k], mod_recv.at[peer], peer, me_t
        ).wait_recv()
    total = mod_sp[0]
    for k in range(1, n_sp):
        total = total + mod_sp[k]
    mod_tp[me_t] = total
    for k in range(1, n_tp):
        peer = lax.rem(me_t + k, n_tp)
        c = remote(
            mod_tp.at[me_t], mod_tp.at[me_t], modt_send.at[k], modt_recv.at[me_t], me_s, peer
        )
        c.start()
        sends.append(c)

    gather_start(wo_view(1), wo_sems(1), wo_source(1))

    for k in range(1, n_tp):
        peer = lax.rem(me_t + k, n_tp)
        remote(
            mod_tp.at[peer], mod_tp.at[peer], modt_send.at[k], modt_recv.at[peer], me_s, peer
        ).wait_recv()

    def vec(r):
        return jnp.concatenate([mod_tp[j][r : r + 1, :] for j in range(n_tp)], axis=1)

    def modulate_rows(first, count, shift, scale):
        def body(i, carry):
            at = pl.ds(pl.multiple_of(first + i * step, step), step)
            hid[at, :] = (x_norm[at, :] * scale + shift).astype(BF16)
            return carry

        lax.fori_loop(0, count // step, body, 0)

    modulate_rows(0, c_rows, vec(1), 1.0 + vec(3))
    modulate_rows(c_rows, rows, vec(0), 1.0 + vec(2))

    head_row = lax.broadcasted_iota(jnp.int32, (width, width), 0) // HEAD_DIM
    head_col = lax.broadcasted_iota(jnp.int32, (width, width), 1) // HEAD_DIM
    same_head = (head_row == head_col).astype(F32)

    def head_scale(p, gain):
        mean = jnp.dot(
            p * p, same_head, precision=lax.Precision.HIGHEST, preferred_element_type=F32
        ) * (1.0 / HEAD_DIM)
        wide_gain = jnp.concatenate([gain[...]] * heads, axis=1)
        return (p * lax.rsqrt(mean + EPS) * wide_gain).astype(BF16)

    own = pl.ds(rows + pl.multiple_of(side * rows, rows), rows)
    other = pl.ds(rows + pl.multiple_of((1 - side) * rows, rows), rows)

    def split(stage, value):
        for h in range(2):
            stage[h] = value[:, h * half : (h + 1) * half]

    def trade(index, stage, block_all, at):
        c = remote(
            stage.at[1 - side], block_all.at[at], pair_send.at[index], pair_recv.at[index],
            mate, me_t,
        )
        c.start()
        sends.append(c)
        return c

    def share_ctx(index, stage, block_ctx):
        block_ctx[me_s] = stage[side]
        for k in range(1, n_sp):
            peer = lax.rem(me_s + k, n_sp)
            c = remote(
                stage.at[lax.rem(peer, 2)], block_ctx.at[me_s],
                ctx_send.at[index, k], ctx_recv.at[index, me_s], peer, me_t,
            )
            c.start()
            sends.append(c)

    def halo_copies(index, block_all):
        down = remote(
            block_all.at[pl.ds(rows, rows)], block_all.at[pl.ds(3 * rows, rows)],
            halo_send.at[index, 0], halo_recv.at[index, 0], me_s - 2, me_t,
        )
        up = remote(
            block_all.at[pl.ds(2 * rows, rows)], block_all.at[pl.ds(0, rows)],
            halo_send.at[index, 1], halo_recv.at[index, 1], me_s + 2, me_t,
        )
        return down, up

    def halo_start(mine):
        for index, block_all in enumerate((k_all, v_all)):
            down, up = halo_copies(index, block_all)
            is_low = side == 0 if mine else side == 1

            @pl.when(is_low & (slab > 0))
            def _():
                down.start()

            @pl.when(jnp.logical_not(is_low) & (slab < last_slab))
            def _():
                up.start()

    copies[5].wait()
    keys = head_scale(jnp.dot(hid[...], w_qkv[0], preferred_element_type=F32), key_gain)
    split(k_stage, keys[c_rows:])
    k_trade = trade(0, k_stage, k_all, own)
    split(ck_stage, keys[:c_rows])
    k_all[own, :] = k_stage[side]
    copies[6].wait()
    values = jnp.dot(hid[...], w_qkv[1], preferred_element_type=F32).astype(BF16)
    split(v_stage, values[c_rows:])
    v_trade = trade(1, v_stage, v_all, own)
    split(cv_stage, values[:c_rows])
    v_all[own, :] = v_stage[side]
    halo_start(True)
    share_ctx(0, ck_stage, ctx_k)
    share_ctx(1, cv_stage, ctx_v)
    copies[7].wait()
    queries = head_scale(
        jnp.dot(hid[c_rows:, :], w_qkv[2], preferred_element_type=F32), query_gain
    ) * jnp.asarray(HEAD_DIM ** (-0.5), BF16)
    split(q_stage, queries)
    q_own = pl.ds(pl.multiple_of(side * rows, rows), rows)
    q_trade = trade(2, q_stage, q_all, q_own)
    q_all[q_own, :] = q_stage[side]
    k_trade.wait_recv()
    v_trade.wait_recv()
    halo_start(False)
    gather_forward(wo_view(0), wo_sems(0))
    q_trade.wait_recv()

    for index, block_ctx in enumerate((ctx_k, ctx_v)):
        for k in range(1, n_sp):
            peer = lax.rem(me_s + k, n_sp)
            remote(
                block_ctx.at[peer], block_ctx.at[peer],
                ctx_send.at[index, k], ctx_recv.at[index, peer], peer, me_t,
            ).wait_recv()
    for index, block_all in enumerate((k_all, v_all)):
        down, up = halo_copies(index, block_all)

        @pl.when(slab < last_slab)
        def _():
            down.wait_recv()

        @pl.when(slab > 0)
        def _():
            up.wait_recv()

    lane_head = lax.broadcasted_iota(jnp.int32, (GRID_W, half), 1) // HEAD_DIM
    masks = [(lane_head == h).astype(F32) for h in range(half_heads)]
    contract_last = (((1,), (1,)), ((), ()))
    all_ck = ctx_k[...].reshape(n_sp * c_rows, half)
    all_cv = ctx_v[...].reshape(n_sp * c_rows, half)

    def attend(i):
        start = jnp.where(
            slab == 0,
            jnp.maximum(i, halo),
            jnp.where(slab == last_slab, jnp.minimum(i, halo), i),
        )
        if last_slab == 0:
            start = jnp.int32(halo)
        at = pl.ds(pl.multiple_of(start * GRID_W, GRID_W), win)
        row_at = pl.ds(pl.multiple_of(i * GRID_W, GRID_W), GRID_W)
        qi = q_all[row_at, :].astype(F32)
        qs = jnp.concatenate([(qi * m).astype(BF16) for m in masks], axis=0)
        s1 = lax.dot_general(qs, k_all[at, :], contract_last, preferred_element_type=F32)
        first = start - i + WIN_ROWS - 1 - halo
        s1 = s1 + jnp.concatenate([table[first + 2 * m] for m in range(WIN_ROWS // 2)], axis=1)
        s2 = lax.dot_general(qs, all_ck, contract_last, preferred_element_type=F32)
        top = jnp.maximum(
            jnp.max(s1, axis=1, keepdims=True), jnp.max(s2, axis=1, keepdims=True)
        )
        e1 = jnp.exp(s1 - top)
        e2 = jnp.exp(s2 - top)
        inv = 1.0 / (jnp.sum(e1, axis=1, keepdims=True) + jnp.sum(e2, axis=1, keepdims=True))
        o = jnp.dot((e1 * inv).astype(BF16), v_all[at, :], preferred_element_type=F32)
        o = o + jnp.dot((e2 * inv).astype(BF16), all_cv, preferred_element_type=F32)
        picked = o[:GRID_W] * masks[0]
        for h in range(1, half_heads):
            picked = picked + o[h * GRID_W : (h + 1) * GRID_W] * masks[h]
        return picked.astype(BF16)

    for i in range(l_rows):
        att_slab[i * GRID_W : (i + 1) * GRID_W, :] = attend((1 - side) * l_rows + i)
    back = remote(
        att_slab, att.at[me_t, side], pair_send.at[3], pair_recv.at[3], mate, me_t
    )
    back.start()
    sends.append(back)
    for i in range(l_rows):
        att[me_t, side, i * GRID_W : (i + 1) * GRID_W, :] = attend(side * l_rows + i)

    back_in = remote(
        att_slab, att.at[me_t, 1 - side], pair_send.at[3], pair_recv.at[3], mate, me_t
    )
    first, second = att_view(side), att_view(1 - side)
    gather_start(first, att_sems(0))
    back_in.wait_recv()
    gather_start(second, att_sems(1))
    gather_forward(first, att_sems(0))
    gather_forward(wo_view(1), wo_sems(1))
    gather_forward(second, att_sems(1))
    copies[8].wait()
    gather_finish(wo_view(0), wo_sems(0))
    gather_finish(wo_view(1), wo_sems(1))
    gather_finish(first, att_sems(0))
    gather_finish(second, att_sems(1))
    gate = vec(4)
    cols = 512
    for n in range(d // cols):
        at = slice(n * cols, (n + 1) * cols)
        branch = jnp.zeros((rows, cols), F32)
        for j in range(n_tp):
            branch = branch + jnp.dot(
                jnp.concatenate([att[j, 0], att[j, 1]], axis=1),
                w_out[j, :, at],
                preferred_element_type=F32,
            ).astype(BF16).astype(F32)
        base = x_in[c_rows:, at].astype(F32)
        out[:, at] = (base + gate[:, at] * branch).astype(BF16)

    for c in sends:
        c.wait_send()
    for index, block_all in enumerate((k_all, v_all)):
        down, up = halo_copies(index, block_all)

        @pl.when(slab > 0)
        def _():
            down.wait_send()

        @pl.when(slab < last_slab)
        def _():
            up.wait_send()


def per_device(
    latent,
    context,
    condition,
    ctx_condition,
    shift_weight,
    scale_weight,
    gate_weight,
    norm_gain,
    query_weight,
    key_weight,
    value_weight,
    query_gain,
    key_gain,
    offset_bias,
    out_weight,
):
    n_sp, n_tp = lax.axis_size("sp"), lax.axis_size("tp")
    rows, d = latent.shape
    c_rows = context.shape[0]
    width = key_weight.shape[1]
    heads = width // HEAD_DIM
    block = shift_weight.shape[1]
    n_pairs = 2 * WIN_ROWS - 2
    half = width // 2
    half_heads = heads // 2
    any_spec = pl.BlockSpec(memory_space=pl.ANY)
    vmem_spec = pl.BlockSpec(memory_space=pltpu.VMEM)
    dma = pltpu.SemaphoreType.DMA
    return pl.pallas_call(
        functools.partial(fused_kernel, n_sp, n_tp),
        out_shape=jax.ShapeDtypeStruct((rows, d), BF16),
        in_specs=[any_spec] * 9 + [vmem_spec] * 6,
        out_specs=vmem_spec,
        scratch_shapes=[
            pltpu.VMEM((rows + c_rows, d), BF16),
            pltpu.VMEM((rows + c_rows, d), F32),
            pltpu.VMEM((rows + c_rows, d), BF16),
            pltpu.VMEM((3, shift_weight.shape[0], block), BF16),
            pltpu.VMEM((3, d, width), BF16),
            pltpu.VMEM((n_tp, width, d), BF16),
            pltpu.VMEM((n_sp, 8, block), F32),
            pltpu.VMEM((n_tp, 8, block), F32),
            pltpu.VMEM((2, rows, half), BF16),
            pltpu.VMEM((2, rows, half), BF16),
            pltpu.VMEM((2, rows, half), BF16),
            pltpu.VMEM((2, c_rows, half), BF16),
            pltpu.VMEM((2, c_rows, half), BF16),
            pltpu.VMEM((2 * rows, half), BF16),
            pltpu.VMEM((4 * rows, half), BF16),
            pltpu.VMEM((4 * rows, half), BF16),
            pltpu.VMEM((n_sp, c_rows, half), BF16),
            pltpu.VMEM((n_sp, c_rows, half), BF16),
            pltpu.VMEM((heads, 2 * WIN_ROWS, 2 * GRID_W), F32),
            pltpu.VMEM((half_heads, 2 * WIN_ROWS, 2 * GRID_W), F32),
            pltpu.VMEM((n_pairs, half_heads * GRID_W, 2 * GRID_W), F32),
            pltpu.VMEM((rows, half), BF16),
            pltpu.VMEM((n_tp, 2, rows, half), BF16),
            dma((9,)),
            dma((n_sp,)),
            dma((n_sp,)),
            dma((n_tp,)),
            dma((n_tp,)),
            dma((4,)),
            dma((4,)),
            dma((2, 2)),
            dma((2, 2)),
            dma((2, n_sp)),
            dma((2, n_sp)),
            dma((2, n_tp)),
            dma((2, n_tp)),
            dma((2, n_tp)),
            dma((2, n_tp)),
        ],
        compiler_params=pltpu.CompilerParams(collective_id=0, has_side_effects=True),
        name="fused_block",
    )(
        latent,
        context,
        shift_weight,
        scale_weight,
        gate_weight,
        query_weight,
        key_weight,
        value_weight,
        out_weight,
        condition.reshape(1, -1),
        ctx_condition.reshape(1, -1),
        norm_gain.reshape(1, -1),
        query_gain.reshape(1, -1),
        key_gain.reshape(1, -1),
        offset_bias,
    )


def fused_fits(latent, context, condition, query_weight, n_sp, n_tp):
    rows, c_rows = latent.shape[0] // n_sp, context.shape[0] // n_sp
    width = query_weight.shape[1] // n_tp
    return (
        rows == WIN_ROWS // 2 * GRID_W
        and c_rows % 32 == 0
        and condition.shape[0] // n_sp % 128 == 0
        and width % 256 == 0
        and n_tp % 2 == 0
        and n_sp % 2 == 0
    )


def solution(mesh):
    in_specs = (
        P("sp", None),
        P("sp", None),
        P("sp"),
        P("sp"),
        P("sp", "tp"),
        P("sp", "tp"),
        P("sp", "tp"),
        P(),
        P(None, "tp"),
        P(None, "tp"),
        P(None, "tp"),
        P(),
        P(),
        P("tp", None, None),
        P("tp", None),
    )
    out_specs = P("sp", None)

    def step(latent, context, condition, ctx_condition, *rest):
        n_sp, n_tp = mesh.shape["sp"], mesh.shape["tp"]
        fits = fused_fits(latent, context, condition, rest[4], n_sp, n_tp)
        body = per_device if fits else per_device_plain
        return jax.shard_map(
            body, mesh=mesh, in_specs=in_specs, out_specs=out_specs, check_vma=False
        )(latent, context, condition, ctx_condition, *rest)

    return step
```

```python
import functools

import jax
import jax.numpy as jnp
from jax import lax
from jax.experimental import pallas as pl
from jax.experimental.pallas import tpu as pltpu
from jax.sharding import PartitionSpec as P

HEAD_DIM = 64
GRID_W = 64
WIN_ROWS = 8
WIN_COLS = 16


EPS = 1e-06


def extended(x, sides, width):
    for axis, dim in sides:
        count, length = (lax.axis_size(axis), x.shape[dim])
        up = [(i, (i + 1) % count) for i in range(count - 1)]
        down = [(j, i) for i, j in up]
        last = lax.slice_in_dim(x, length - width, length, axis=dim)
        initial = lax.slice_in_dim(x, 0, width, axis=dim)
        before = lax.ppermute(last, axis, up)
        after = lax.ppermute(initial, axis, down)
        x = jnp.concatenate([before, x, after], axis=dim)
    return x


def modulate(rows_in, norm_gain, shift_vec, scale_vec):
    values = rows_in.astype(jnp.float32)
    normed = values * lax.rsqrt(jnp.mean(values * values, axis=-1, keepdims=True) + EPS)
    return (normed * norm_gain * (1.0 + scale_vec) + shift_vec).astype(jnp.bfloat16)


def head_norm(projected, head_gain):
    row_count = projected.shape[0]
    split_heads = projected.reshape(row_count, -1, head_gain.shape[0])
    normed = split_heads * lax.rsqrt(
        jnp.mean(split_heads * split_heads, axis=-1, keepdims=True) + EPS
    )
    return (normed * head_gain).astype(jnp.bfloat16).reshape(row_count, -1)


def per_device_plain(
    latent,
    context,
    condition,
    ctx_condition,
    shift_weight,
    scale_weight,
    gate_weight,
    norm_gain,
    query_weight,
    key_weight,
    value_weight,
    query_gain,
    key_gain,
    offset_bias,
    out_weight,
):
    activations = jax.nn.silu(jnp.stack([condition, ctx_condition])).astype(jnp.bfloat16)
    part_shift = jnp.dot(activations, shift_weight, preferred_element_type=jnp.float32)
    part_scale = jnp.dot(activations, scale_weight, preferred_element_type=jnp.float32)
    part_gate = jnp.dot(activations[:1], gate_weight, preferred_element_type=jnp.float32)
    block_cols = shift_weight.shape[1]
    first_col = lax.axis_index("tp") * block_cols

    def spread(piece_part):
        padded_vec = jnp.zeros((piece_part.shape[0], block_cols * lax.axis_size("tp")), jnp.float32)
        return lax.dynamic_update_slice_in_dim(padded_vec, piece_part, first_col, 1)

    shift_vec, scale_vec, gate_vec = lax.psum(
        (spread(part_shift), spread(part_scale), spread(part_gate)), ("sp", "tp")
    )
    hidden = modulate(latent, norm_gain, shift_vec[0], scale_vec[0])
    queries = head_norm(
        jnp.dot(hidden, query_weight, preferred_element_type=jnp.float32), query_gain
    )
    keys_lat = head_norm(jnp.dot(hidden, key_weight, preferred_element_type=jnp.float32), key_gain)
    values_lat = jnp.dot(hidden, value_weight, preferred_element_type=jnp.float32).astype(
        jnp.bfloat16
    )
    ctx_hidden = modulate(
        lax.all_gather(context, "sp", axis=0, tiled=True), norm_gain, shift_vec[1], scale_vec[1]
    )
    ctx_keys = head_norm(
        jnp.dot(ctx_hidden, key_weight, preferred_element_type=jnp.float32), key_gain
    )
    ctx_values = jnp.dot(ctx_hidden, value_weight, preferred_element_type=jnp.float32).astype(
        jnp.bfloat16
    )
    ctx_pairs = jnp.concatenate([ctx_keys, ctx_values], axis=1)
    col_width = keys_lat.shape[1]
    heads_dev = col_width // HEAD_DIM
    local_rows = keys_lat.shape[0] // GRID_W
    halo_rows = WIN_ROWS // 2
    window_keys = WIN_ROWS * GRID_W
    key_value = jnp.concatenate([keys_lat, values_lat], axis=1).reshape(
        local_rows, GRID_W, 2 * col_width
    )
    padded = extended(key_value, (("sp", 0),), halo_rows)
    first_row = lax.axis_index("sp") * local_rows
    total_rows = local_rows * lax.axis_size("sp")
    global_rows = first_row + jnp.arange(local_rows, dtype=jnp.int32)
    band_start = jnp.clip(global_rows - halo_rows, 0, total_rows - WIN_ROWS)
    band_global = band_start[:, None] + jnp.arange(WIN_ROWS, dtype=jnp.int32)[None, :]
    banded = jnp.take(padded, band_global - first_row + halo_rows, axis=0)
    key_band = banded[..., :col_width].reshape(local_rows, window_keys, heads_dev, HEAD_DIM)
    value_band = banded[..., col_width:].reshape(local_rows, window_keys, heads_dev, HEAD_DIM)
    row_steps = band_global - global_rows[:, None] + WIN_ROWS - 1
    row_hot = (
        row_steps[:, :, None] == jnp.arange(2 * WIN_ROWS - 1, dtype=jnp.int32)[None, None, :]
    ).astype(jnp.float32)
    column_ids = jnp.arange(GRID_W, dtype=jnp.int32)
    col_steps = (
        jnp.clip(column_ids[None, :] - column_ids[:, None], 1 - WIN_COLS, WIN_COLS - 1)
        + WIN_COLS
        - 1
    )
    col_hot = (
        col_steps[:, :, None] == jnp.arange(2 * WIN_COLS - 1, dtype=jnp.int32)[None, None, :]
    ).astype(jnp.float32)
    col_start = jnp.clip(column_ids - WIN_COLS // 2, 0, GRID_W - WIN_COLS)
    col_open = (column_ids[None, :] >= col_start[:, None]) & (
        column_ids[None, :] < col_start[:, None] + WIN_COLS
    )
    col_table = jnp.einsum("hab,qkb->haqk", offset_bias, col_hot, precision=lax.Precision.HIGHEST)
    col_table = jnp.where(col_open[None, None, :, :], col_table, -jnp.inf)
    offset_terms = jnp.einsum(
        "rja,haqk->hrqjk",
        row_hot,
        jnp.where(col_open[None, None], col_table, 0.0),
        precision=lax.Precision.HIGHEST,
    )
    offset_terms = jnp.where(col_open[None, None, :, None, :], offset_terms, -jnp.inf)
    offset_terms = offset_terms.reshape(heads_dev, local_rows, GRID_W, window_keys)
    score_scale = HEAD_DIM ** (-0.5)
    q_grid = queries.reshape(local_rows, GRID_W, heads_dev, HEAD_DIM)
    scores = (
        jnp.einsum("rqhd,rnhd->hrqn", q_grid, key_band, preferred_element_type=jnp.float32)
        * score_scale
        + offset_terms
    )
    ctx_count = ctx_pairs.shape[0]
    ctx_keys_all = ctx_pairs[:, :col_width].reshape(ctx_count, heads_dev, HEAD_DIM)
    ctx_values_all = ctx_pairs[:, col_width:].reshape(ctx_count, heads_dev, HEAD_DIM)
    ctx_scores = (
        jnp.einsum("rqhd,nhd->hrqn", q_grid, ctx_keys_all, preferred_element_type=jnp.float32)
        * score_scale
    )
    row_max = jnp.maximum(jnp.max(scores, axis=3), jnp.max(ctx_scores, axis=3))
    local_exp = jnp.exp(scores - row_max[..., None])
    ctx_exp = jnp.exp(ctx_scores - row_max[..., None])
    denominator = jnp.sum(local_exp, axis=3) + jnp.sum(ctx_exp, axis=3)
    local_weights = (local_exp / denominator[..., None]).astype(jnp.bfloat16)
    ctx_weights = (ctx_exp / denominator[..., None]).astype(jnp.bfloat16)
    combined = jnp.einsum(
        "hrqn,rnhd->rqhd", local_weights, value_band, preferred_element_type=jnp.float32
    ) + jnp.einsum(
        "hrqn,nhd->rqhd", ctx_weights, ctx_values_all, preferred_element_type=jnp.float32
    )
    attended = combined.astype(jnp.bfloat16).reshape(local_rows * GRID_W, col_width)
    partial_value = jnp.dot(attended, out_weight, preferred_element_type=jnp.float32)
    branch = lax.psum(partial_value.astype(jnp.bfloat16), "tp").astype(jnp.float32)
    return (latent.astype(jnp.float32) + gate_vec[0] * branch).astype(jnp.bfloat16)


MESH = pl.DeviceIdType.MESH
MASKED = -1e30
F32 = jnp.float32
BF16 = jnp.bfloat16


def fused_kernel(
    n_sp,
    n_tp,
    latent,
    context,
    shift_w,
    scale_w,
    gate_w,
    query_w,
    key_w,
    value_w,
    out_w,
    cond,
    ctx_cond,
    norm_gain,
    query_gain,
    key_gain,
    bias_in,
    out,
    x_in,
    x_norm,
    hid,
    w_mod,
    w_qkv,
    w_out,
    mod_sp,
    mod_tp,
    q_stage,
    k_stage,
    v_stage,
    ck_stage,
    cv_stage,
    q_all,
    k_all,
    v_all,
    ctx_k,
    ctx_v,
    bias_pad,
    bias_lines,
    table,
    att_slab,
    att,
    local_sem,
    mod_send,
    mod_recv,
    modt_send,
    modt_recv,
    pair_send,
    pair_recv,
    halo_send,
    halo_recv,
    ctx_send,
    ctx_recv,
    wo_send,
    wo_recv,
    att_send,
    att_recv,
):
    me_s, me_t = lax.axis_index("sp"), lax.axis_index("tp")
    rows, d = latent.shape
    c_rows = context.shape[0]
    width = key_w.shape[1]
    heads = width // HEAD_DIM
    block = shift_w.shape[1]
    l_rows = rows // GRID_W
    halo = WIN_ROWS // 2
    win = WIN_ROWS * GRID_W
    core = lax.rem(me_t, 2)
    chip = lax.div(me_t, 2)
    partner = me_t + 1 - 2 * core
    n_x = n_tp // 2
    side = lax.rem(me_s, 2)
    slab = lax.div(me_s, 2)
    mate = me_s + 1 - 2 * side
    last_slab = n_sp // 2 - 1
    half = width // 2
    half_heads = heads // 2

    def remote(src, dst, send, recv, s, t):
        return pltpu.make_async_remote_copy(
            src_ref=src, dst_ref=dst, send_sem=send, recv_sem=recv,
            device_id=(s, t), device_id_type=MESH,
        )

    barrier = pltpu.get_barrier_semaphore()
    for k in range(1, n_sp):
        pl.semaphore_signal(
            barrier, inc=1, device_id=(lax.rem(me_s + k, n_sp), me_t), device_id_type=MESH
        )
    for k in range(1, n_tp):
        pl.semaphore_signal(
            barrier, inc=1, device_id=(me_s, lax.rem(me_t + k, n_tp)), device_id_type=MESH
        )

    loads = [
        (shift_w, w_mod.at[0]),
        (scale_w, w_mod.at[1]),
        (gate_w, w_mod.at[2]),
        (context, x_in.at[pl.ds(0, c_rows)]),
        (latent, x_in.at[pl.ds(c_rows, rows)]),
        (key_w, w_qkv.at[0]),
        (value_w, w_qkv.at[1]),
        (query_w, w_qkv.at[2]),
        (out_w, w_out.at[me_t]),
    ]
    copies = [pltpu.make_async_copy(a, b, local_sem.at[i]) for i, (a, b) in enumerate(loads)]
    for c in copies[:3]:
        c.start()

    def silu(v):
        return v / (1.0 + jnp.exp(-v))

    two = (16, cond.shape[1])
    row_id = lax.broadcasted_iota(jnp.int32, two, 0)
    act0 = jnp.broadcast_to(silu(cond[...]), two)
    act1 = jnp.broadcast_to(silu(ctx_cond[...]), two)

    def placed(first, second):
        picked = jnp.where(row_id == first, act0, 0.0)
        if second is not None:
            picked = jnp.where(row_id == second, act1, picked)
        return picked.astype(BF16)

    part = jnp.zeros((16, block), F32)
    for i, (first, second) in enumerate(((0, 1), (2, 3), (4, None))):
        copies[i].wait()
        part += jnp.dot(placed(first, second), w_mod[i], preferred_element_type=F32)
    for c in copies[3:]:
        c.start()
    mod_sp[me_s] = part[:8]
    pl.semaphore_wait(barrier, n_sp + n_tp - 2)
    sends = []
    for k in range(1, n_sp):
        peer = lax.rem(me_s + k, n_sp)
        c = remote(
            mod_sp.at[me_s], mod_sp.at[me_s], mod_send.at[k], mod_recv.at[me_s], peer, me_t
        )
        c.start()
        sends.append(c)

    def gather_start(view, sems, source=None):
        send, recv = sems
        mine = view(me_t) if source is None else source
        started = [remote(mine, view(me_t), send(0), recv(me_t), me_s, partner)]
        for k in range(1, n_x):
            far = 2 * lax.rem(chip + k, n_x) + core
            started.append(remote(mine, view(me_t), send(k), recv(me_t), me_s, far))
        for c in reversed(started):
            c.start()
        sends.extend(started)

    def gather_forward(view, sems):
        send, recv = sems
        for k in range(1, n_x):
            came = 2 * lax.rem(chip + n_x - k, n_x) + core
            c = remote(view(came), view(came), send(n_x + k), recv(came), me_s, partner)
            c.wait_recv()
            c.start()
            sends.append(c)

    def gather_finish(view, sems):
        send, recv = sems
        remote(
            view(partner), view(partner), send(0), recv(partner), me_s, partner
        ).wait_recv()
        for k in range(1, n_x):
            came = 2 * lax.rem(chip + n_x - k, n_x) + 1 - core
            remote(
                view(came), view(came), send(n_x + k), recv(came), me_s, partner
            ).wait_recv()

    early = width // 4
    wo_rows = (pl.ds(0, early), pl.ds(early, width - early))

    def wo_view(c):
        return lambda j: w_out.at[j, wo_rows[c]]

    def wo_source(c):
        return out_w.at[wo_rows[c]]

    def wo_sems(c):
        return (lambda k: wo_send.at[c, k]), (lambda k: wo_recv.at[c, k])

    def att_view(h):
        return lambda j: att.at[j, h]

    def att_sems(n):
        return (lambda k: att_send.at[n, k]), (lambda k: att_recv.at[n, k])

    gather_start(wo_view(0), wo_sems(0), wo_source(0))

    copies[3].wait()
    copies[4].wait()
    step = 32

    def norm_rows(i, carry):
        at = pl.ds(pl.multiple_of(i * step, step), step)
        v = x_in[at, :].astype(F32)
        r = lax.rsqrt(jnp.mean(v * v, axis=-1, keepdims=True) + EPS)
        x_norm[at, :] = v * r * norm_gain[...]
        return carry

    lax.fori_loop(0, (rows + c_rows) // step, norm_rows, 0)

    pair = 2 * GRID_W
    q_col = lax.broadcasted_iota(jnp.int32, (GRID_W, pair), 0)
    k_col = lax.broadcasted_iota(jnp.int32, (GRID_W, pair), 1) % GRID_W
    col0 = jnp.clip(q_col - WIN_COLS // 2, 0, GRID_W - WIN_COLS)
    col_open = (k_col >= col0) & (k_col < col0 + WIN_COLS)
    n_pairs = 2 * WIN_ROWS - 2
    bias_pad[...] = jnp.zeros_like(bias_pad)
    for h in range(heads):
        bias_pad[h, : 2 * WIN_ROWS - 1, : 2 * WIN_COLS - 1] = bias_in[:, h, :]
    for h in range(half_heads):
        head = side * half_heads + h
        upper = pltpu.roll(bias_pad[head, 1 : n_pairs + 1, :], GRID_W, 1)
        bias_lines[h, :n_pairs, :] = bias_pad[head, :n_pairs, :] + upper
        for a in range(n_pairs):
            line = jnp.broadcast_to(bias_lines[h, a : a + 1, :], (GRID_W, pair))
            rolled = pltpu.roll(line, pair - (WIN_COLS - 1), 1, stride=1, stride_axis=0)
            table[a, h * GRID_W : (h + 1) * GRID_W, :] = jnp.where(col_open, rolled, MASKED)

    for k in range(1, n_sp):
        peer = lax.rem(me_s + k, n_sp)
        remote(
            mod_sp.at[peer], mod_sp.at[peer], mod_send.at[k], mod_recv.at[peer], peer, me_t
        ).wait_recv()
    total = mod_sp[0]
    for k in range(1, n_sp):
        total = total + mod_sp[k]
    mod_tp[me_t] = total
    for k in range(1, n_tp):
        peer = lax.rem(me_t + k, n_tp)
        c = remote(
            mod_tp.at[me_t], mod_tp.at[me_t], modt_send.at[k], modt_recv.at[me_t], me_s, peer
        )
        c.start()
        sends.append(c)

    gather_start(wo_view(1), wo_sems(1), wo_source(1))

    for k in range(1, n_tp):
        peer = lax.rem(me_t + k, n_tp)
        remote(
            mod_tp.at[peer], mod_tp.at[peer], modt_send.at[k], modt_recv.at[peer], me_s, peer
        ).wait_recv()

    def vec(r):
        return jnp.concatenate([mod_tp[j][r : r + 1, :] for j in range(n_tp)], axis=1)

    def modulate_rows(first, count, shift, scale):
        def body(i, carry):
            at = pl.ds(pl.multiple_of(first + i * step, step), step)
            hid[at, :] = (x_norm[at, :] * scale + shift).astype(BF16)
            return carry

        lax.fori_loop(0, count // step, body, 0)

    modulate_rows(0, c_rows, vec(1), 1.0 + vec(3))
    modulate_rows(c_rows, rows, vec(0), 1.0 + vec(2))

    head_row = lax.broadcasted_iota(jnp.int32, (width, width), 0) // HEAD_DIM
    head_col = lax.broadcasted_iota(jnp.int32, (width, width), 1) // HEAD_DIM
    same_head = (head_row == head_col).astype(F32)

    def head_scale(p, gain):
        mean = jnp.dot(
            p * p, same_head, precision=lax.Precision.HIGHEST, preferred_element_type=F32
        ) * (1.0 / HEAD_DIM)
        wide_gain = jnp.concatenate([gain[...]] * heads, axis=1)
        return (p * lax.rsqrt(mean + EPS) * wide_gain).astype(BF16)

    own = pl.ds(rows + pl.multiple_of(side * rows, rows), rows)
    other = pl.ds(rows + pl.multiple_of((1 - side) * rows, rows), rows)

    def split(stage, value):
        for h in range(2):
            stage[h] = value[:, h * half : (h + 1) * half]

    def trade(index, stage, block_all, at):
        c = remote(
            stage.at[1 - side], block_all.at[at], pair_send.at[index], pair_recv.at[index],
            mate, me_t,
        )
        c.start()
        sends.append(c)
        return c

    def share_ctx(index, stage, block_ctx):
        block_ctx[me_s] = stage[side]
        for k in range(1, n_sp):
            peer = lax.rem(me_s + k, n_sp)
            c = remote(
                stage.at[lax.rem(peer, 2)], block_ctx.at[me_s],
                ctx_send.at[index, k], ctx_recv.at[index, me_s], peer, me_t,
            )
            c.start()
            sends.append(c)

    def halo_copies(index, block_all):
        down = remote(
            block_all.at[pl.ds(rows, rows)], block_all.at[pl.ds(3 * rows, rows)],
            halo_send.at[index, 0], halo_recv.at[index, 0], me_s - 2, me_t,
        )
        up = remote(
            block_all.at[pl.ds(2 * rows, rows)], block_all.at[pl.ds(0, rows)],
            halo_send.at[index, 1], halo_recv.at[index, 1], me_s + 2, me_t,
        )
        return down, up

    def halo_start(mine):
        for index, block_all in enumerate((k_all, v_all)):
            down, up = halo_copies(index, block_all)
            is_low = side == 0 if mine else side == 1

            @pl.when(is_low & (slab > 0))
            def _():
                down.start()

            @pl.when(jnp.logical_not(is_low) & (slab < last_slab))
            def _():
                up.start()

    copies[5].wait()
    keys = head_scale(jnp.dot(hid[...], w_qkv[0], preferred_element_type=F32), key_gain)
    split(k_stage, keys[c_rows:])
    k_trade = trade(0, k_stage, k_all, own)
    split(ck_stage, keys[:c_rows])
    k_all[own, :] = k_stage[side]
    copies[6].wait()
    values = jnp.dot(hid[...], w_qkv[1], preferred_element_type=F32).astype(BF16)
    split(v_stage, values[c_rows:])
    v_trade = trade(1, v_stage, v_all, own)
    split(cv_stage, values[:c_rows])
    v_all[own, :] = v_stage[side]
    halo_start(True)
    share_ctx(0, ck_stage, ctx_k)
    share_ctx(1, cv_stage, ctx_v)
    copies[7].wait()
    queries = head_scale(
        jnp.dot(hid[c_rows:, :], w_qkv[2], preferred_element_type=F32), query_gain
    ) * jnp.asarray(HEAD_DIM ** (-0.5), BF16)
    split(q_stage, queries)
    q_own = pl.ds(pl.multiple_of(side * rows, rows), rows)
    q_trade = trade(2, q_stage, q_all, q_own)
    q_all[q_own, :] = q_stage[side]
    k_trade.wait_recv()
    v_trade.wait_recv()
    halo_start(False)
    gather_forward(wo_view(0), wo_sems(0))
    q_trade.wait_recv()

    for index, block_ctx in enumerate((ctx_k, ctx_v)):
        for k in range(1, n_sp):
            peer = lax.rem(me_s + k, n_sp)
            remote(
                block_ctx.at[peer], block_ctx.at[peer],
                ctx_send.at[index, k], ctx_recv.at[index, peer], peer, me_t,
            ).wait_recv()
    for index, block_all in enumerate((k_all, v_all)):
        down, up = halo_copies(index, block_all)

        @pl.when(slab < last_slab)
        def _():
            down.wait_recv()

        @pl.when(slab > 0)
        def _():
            up.wait_recv()

    lane_head = lax.broadcasted_iota(jnp.int32, (GRID_W, half), 1) // HEAD_DIM
    masks = [(lane_head == h).astype(F32) for h in range(half_heads)]
    contract_last = (((1,), (1,)), ((), ()))
    all_ck = ctx_k[...].reshape(n_sp * c_rows, half)
    all_cv = ctx_v[...].reshape(n_sp * c_rows, half)

    def attend(i):
        start = jnp.where(
            slab == 0,
            jnp.maximum(i, halo),
            jnp.where(slab == last_slab, jnp.minimum(i, halo), i),
        )
        if last_slab == 0:
            start = jnp.int32(halo)
        at = pl.ds(pl.multiple_of(start * GRID_W, GRID_W), win)
        row_at = pl.ds(pl.multiple_of(i * GRID_W, GRID_W), GRID_W)
        qi = q_all[row_at, :].astype(F32)
        qs = jnp.concatenate([(qi * m).astype(BF16) for m in masks], axis=0)
        s1 = lax.dot_general(qs, k_all[at, :], contract_last, preferred_element_type=F32)
        first = start - i + WIN_ROWS - 1 - halo
        s1 = s1 + jnp.concatenate([table[first + 2 * m] for m in range(WIN_ROWS // 2)], axis=1)
        s2 = lax.dot_general(qs, all_ck, contract_last, preferred_element_type=F32)
        top = jnp.maximum(
            jnp.max(s1, axis=1, keepdims=True), jnp.max(s2, axis=1, keepdims=True)
        )
        e1 = jnp.exp(s1 - top)
        e2 = jnp.exp(s2 - top)
        inv = 1.0 / (jnp.sum(e1, axis=1, keepdims=True) + jnp.sum(e2, axis=1, keepdims=True))
        o = jnp.dot((e1 * inv).astype(BF16), v_all[at, :], preferred_element_type=F32)
        o = o + jnp.dot((e2 * inv).astype(BF16), all_cv, preferred_element_type=F32)
        picked = o[:GRID_W] * masks[0]
        for h in range(1, half_heads):
            picked = picked + o[h * GRID_W : (h + 1) * GRID_W] * masks[h]
        return picked.astype(BF16)

    for i in range(l_rows):
        att_slab[i * GRID_W : (i + 1) * GRID_W, :] = attend((1 - side) * l_rows + i)
    back = remote(
        att_slab, att.at[me_t, side], pair_send.at[3], pair_recv.at[3], mate, me_t
    )
    back.start()
    sends.append(back)
    for i in range(l_rows):
        att[me_t, side, i * GRID_W : (i + 1) * GRID_W, :] = attend(side * l_rows + i)

    back_in = remote(
        att_slab, att.at[me_t, 1 - side], pair_send.at[3], pair_recv.at[3], mate, me_t
    )
    first, second = att_view(side), att_view(1 - side)
    gather_start(first, att_sems(0))
    back_in.wait_recv()
    gather_start(second, att_sems(1))
    gather_forward(first, att_sems(0))
    gather_forward(wo_view(1), wo_sems(1))
    gather_forward(second, att_sems(1))
    copies[8].wait()
    gather_finish(wo_view(0), wo_sems(0))
    gather_finish(wo_view(1), wo_sems(1))
    gather_finish(first, att_sems(0))
    gather_finish(second, att_sems(1))
    gate = vec(4)
    cols = 512
    for n in range(d // cols):
        at = slice(n * cols, (n + 1) * cols)
        branch = jnp.zeros((rows, cols), F32)
        for j in range(n_tp):
            branch = branch + jnp.dot(
                jnp.concatenate([att[j, 0], att[j, 1]], axis=1),
                w_out[j, :, at],
                preferred_element_type=F32,
            ).astype(BF16).astype(F32)
        base = x_in[c_rows:, at].astype(F32)
        out[:, at] = (base + gate[:, at] * branch).astype(BF16)

    for c in sends:
        c.wait_send()
    for index, block_all in enumerate((k_all, v_all)):
        down, up = halo_copies(index, block_all)

        @pl.when(slab > 0)
        def _():
            down.wait_send()

        @pl.when(slab < last_slab)
        def _():
            up.wait_send()


def per_device(
    latent,
    context,
    condition,
    ctx_condition,
    shift_weight,
    scale_weight,
    gate_weight,
    norm_gain,
    query_weight,
    key_weight,
    value_weight,
    query_gain,
    key_gain,
    offset_bias,
    out_weight,
):
    n_sp, n_tp = lax.axis_size("sp"), lax.axis_size("tp")
    rows, d = latent.shape
    c_rows = context.shape[0]
    width = key_weight.shape[1]
    heads = width // HEAD_DIM
    block = shift_weight.shape[1]
    n_pairs = 2 * WIN_ROWS - 2
    half = width // 2
    half_heads = heads // 2
    any_spec = pl.BlockSpec(memory_space=pl.ANY)
    vmem_spec = pl.BlockSpec(memory_space=pltpu.VMEM)
    dma = pltpu.SemaphoreType.DMA
    return pl.pallas_call(
        functools.partial(fused_kernel, n_sp, n_tp),
        out_shape=pltpu.VMEM((rows, d), BF16),
        in_specs=[any_spec] * 9 + [vmem_spec] * 6,
        out_specs=vmem_spec,
        scratch_shapes=[
            pltpu.VMEM((rows + c_rows, d), BF16),
            pltpu.VMEM((rows + c_rows, d), F32),
            pltpu.VMEM((rows + c_rows, d), BF16),
            pltpu.VMEM((3, shift_weight.shape[0], block), BF16),
            pltpu.VMEM((3, d, width), BF16),
            pltpu.VMEM((n_tp, width, d), BF16),
            pltpu.VMEM((n_sp, 8, block), F32),
            pltpu.VMEM((n_tp, 8, block), F32),
            pltpu.VMEM((2, rows, half), BF16),
            pltpu.VMEM((2, rows, half), BF16),
            pltpu.VMEM((2, rows, half), BF16),
            pltpu.VMEM((2, c_rows, half), BF16),
            pltpu.VMEM((2, c_rows, half), BF16),
            pltpu.VMEM((2 * rows, half), BF16),
            pltpu.VMEM((4 * rows, half), BF16),
            pltpu.VMEM((4 * rows, half), BF16),
            pltpu.VMEM((n_sp, c_rows, half), BF16),
            pltpu.VMEM((n_sp, c_rows, half), BF16),
            pltpu.VMEM((heads, 2 * WIN_ROWS, 2 * GRID_W), F32),
            pltpu.VMEM((half_heads, 2 * WIN_ROWS, 2 * GRID_W), F32),
            pltpu.VMEM((n_pairs, half_heads * GRID_W, 2 * GRID_W), F32),
            pltpu.VMEM((rows, half), BF16),
            pltpu.VMEM((n_tp, 2, rows, half), BF16),
            dma((9,)),
            dma((n_sp,)),
            dma((n_sp,)),
            dma((n_tp,)),
            dma((n_tp,)),
            dma((4,)),
            dma((4,)),
            dma((2, 2)),
            dma((2, 2)),
            dma((2, n_sp)),
            dma((2, n_sp)),
            dma((2, n_tp)),
            dma((2, n_tp)),
            dma((2, n_tp)),
            dma((2, n_tp)),
        ],
        compiler_params=pltpu.CompilerParams(collective_id=0, has_side_effects=True),
        name="fused_block",
    )(
        latent,
        context,
        shift_weight,
        scale_weight,
        gate_weight,
        query_weight,
        key_weight,
        value_weight,
        out_weight,
        condition.reshape(1, -1),
        ctx_condition.reshape(1, -1),
        norm_gain.reshape(1, -1),
        query_gain.reshape(1, -1),
        key_gain.reshape(1, -1),
        offset_bias.transpose(1, 0, 2),
    )


def fused_fits(latent, context, condition, query_weight, n_sp, n_tp):
    rows, c_rows = latent.shape[0] // n_sp, context.shape[0] // n_sp
    width = query_weight.shape[1] // n_tp
    return (
        rows == WIN_ROWS // 2 * GRID_W
        and c_rows % 32 == 0
        and condition.shape[0] // n_sp % 128 == 0
        and width % 256 == 0
        and n_tp % 2 == 0
        and n_sp % 2 == 0
    )


def solution(mesh):
    in_specs = (
        P("sp", None),
        P("sp", None),
        P("sp"),
        P("sp"),
        P("sp", "tp"),
        P("sp", "tp"),
        P("sp", "tp"),
        P(),
        P(None, "tp"),
        P(None, "tp"),
        P(None, "tp"),
        P(),
        P(),
        P("tp", None, None),
        P("tp", None),
    )
    out_specs = P("sp", None)

    def step(latent, context, condition, ctx_condition, *rest):
        n_sp, n_tp = mesh.shape["sp"], mesh.shape["tp"]
        fits = fused_fits(latent, context, condition, rest[4], n_sp, n_tp)
        body = per_device if fits else per_device_plain
        return jax.shard_map(
            body, mesh=mesh, in_specs=in_specs, out_specs=out_specs, check_vma=False
        )(latent, context, condition, ctx_condition, *rest)

    return step
```

```python
import functools

import jax
import jax.numpy as jnp
from jax import lax
from jax.experimental import pallas as pl
from jax.experimental.pallas import tpu as pltpu
from jax.sharding import PartitionSpec as P

HEAD_DIM = 64
GRID_W = 64
WIN_ROWS = 8
WIN_COLS = 16


EPS = 1e-06


def extended(x, sides, width):
    for axis, dim in sides:
        count, length = (lax.axis_size(axis), x.shape[dim])
        up = [(i, (i + 1) % count) for i in range(count - 1)]
        down = [(j, i) for i, j in up]
        last = lax.slice_in_dim(x, length - width, length, axis=dim)
        initial = lax.slice_in_dim(x, 0, width, axis=dim)
        before = lax.ppermute(last, axis, up)
        after = lax.ppermute(initial, axis, down)
        x = jnp.concatenate([before, x, after], axis=dim)
    return x


def modulate(rows_in, norm_gain, shift_vec, scale_vec):
    values = rows_in.astype(jnp.float32)
    normed = values * lax.rsqrt(jnp.mean(values * values, axis=-1, keepdims=True) + EPS)
    return (normed * norm_gain * (1.0 + scale_vec) + shift_vec).astype(jnp.bfloat16)


def head_norm(projected, head_gain):
    row_count = projected.shape[0]
    split_heads = projected.reshape(row_count, -1, head_gain.shape[0])
    normed = split_heads * lax.rsqrt(
        jnp.mean(split_heads * split_heads, axis=-1, keepdims=True) + EPS
    )
    return (normed * head_gain).astype(jnp.bfloat16).reshape(row_count, -1)


def per_device_plain(
    latent,
    context,
    condition,
    ctx_condition,
    shift_weight,
    scale_weight,
    gate_weight,
    norm_gain,
    query_weight,
    key_weight,
    value_weight,
    query_gain,
    key_gain,
    offset_bias,
    out_weight,
):
    activations = jax.nn.silu(jnp.stack([condition, ctx_condition])).astype(jnp.bfloat16)
    part_shift = jnp.dot(activations, shift_weight, preferred_element_type=jnp.float32)
    part_scale = jnp.dot(activations, scale_weight, preferred_element_type=jnp.float32)
    part_gate = jnp.dot(activations[:1], gate_weight, preferred_element_type=jnp.float32)
    block_cols = shift_weight.shape[1]
    first_col = lax.axis_index("tp") * block_cols

    def spread(piece_part):
        padded_vec = jnp.zeros((piece_part.shape[0], block_cols * lax.axis_size("tp")), jnp.float32)
        return lax.dynamic_update_slice_in_dim(padded_vec, piece_part, first_col, 1)

    shift_vec, scale_vec, gate_vec = lax.psum(
        (spread(part_shift), spread(part_scale), spread(part_gate)), ("sp", "tp")
    )
    hidden = modulate(latent, norm_gain, shift_vec[0], scale_vec[0])
    queries = head_norm(
        jnp.dot(hidden, query_weight, preferred_element_type=jnp.float32), query_gain
    )
    keys_lat = head_norm(jnp.dot(hidden, key_weight, preferred_element_type=jnp.float32), key_gain)
    values_lat = jnp.dot(hidden, value_weight, preferred_element_type=jnp.float32).astype(
        jnp.bfloat16
    )
    ctx_hidden = modulate(
        lax.all_gather(context, "sp", axis=0, tiled=True), norm_gain, shift_vec[1], scale_vec[1]
    )
    ctx_keys = head_norm(
        jnp.dot(ctx_hidden, key_weight, preferred_element_type=jnp.float32), key_gain
    )
    ctx_values = jnp.dot(ctx_hidden, value_weight, preferred_element_type=jnp.float32).astype(
        jnp.bfloat16
    )
    ctx_pairs = jnp.concatenate([ctx_keys, ctx_values], axis=1)
    col_width = keys_lat.shape[1]
    heads_dev = col_width // HEAD_DIM
    local_rows = keys_lat.shape[0] // GRID_W
    halo_rows = WIN_ROWS // 2
    window_keys = WIN_ROWS * GRID_W
    key_value = jnp.concatenate([keys_lat, values_lat], axis=1).reshape(
        local_rows, GRID_W, 2 * col_width
    )
    padded = extended(key_value, (("sp", 0),), halo_rows)
    first_row = lax.axis_index("sp") * local_rows
    total_rows = local_rows * lax.axis_size("sp")
    global_rows = first_row + jnp.arange(local_rows, dtype=jnp.int32)
    band_start = jnp.clip(global_rows - halo_rows, 0, total_rows - WIN_ROWS)
    band_global = band_start[:, None] + jnp.arange(WIN_ROWS, dtype=jnp.int32)[None, :]
    banded = jnp.take(padded, band_global - first_row + halo_rows, axis=0)
    key_band = banded[..., :col_width].reshape(local_rows, window_keys, heads_dev, HEAD_DIM)
    value_band = banded[..., col_width:].reshape(local_rows, window_keys, heads_dev, HEAD_DIM)
    row_steps = band_global - global_rows[:, None] + WIN_ROWS - 1
    row_hot = (
        row_steps[:, :, None] == jnp.arange(2 * WIN_ROWS - 1, dtype=jnp.int32)[None, None, :]
    ).astype(jnp.float32)
    column_ids = jnp.arange(GRID_W, dtype=jnp.int32)
    col_steps = (
        jnp.clip(column_ids[None, :] - column_ids[:, None], 1 - WIN_COLS, WIN_COLS - 1)
        + WIN_COLS
        - 1
    )
    col_hot = (
        col_steps[:, :, None] == jnp.arange(2 * WIN_COLS - 1, dtype=jnp.int32)[None, None, :]
    ).astype(jnp.float32)
    col_start = jnp.clip(column_ids - WIN_COLS // 2, 0, GRID_W - WIN_COLS)
    col_open = (column_ids[None, :] >= col_start[:, None]) & (
        column_ids[None, :] < col_start[:, None] + WIN_COLS
    )
    col_table = jnp.einsum("hab,qkb->haqk", offset_bias, col_hot, precision=lax.Precision.HIGHEST)
    col_table = jnp.where(col_open[None, None, :, :], col_table, -jnp.inf)
    offset_terms = jnp.einsum(
        "rja,haqk->hrqjk",
        row_hot,
        jnp.where(col_open[None, None], col_table, 0.0),
        precision=lax.Precision.HIGHEST,
    )
    offset_terms = jnp.where(col_open[None, None, :, None, :], offset_terms, -jnp.inf)
    offset_terms = offset_terms.reshape(heads_dev, local_rows, GRID_W, window_keys)
    score_scale = HEAD_DIM ** (-0.5)
    q_grid = queries.reshape(local_rows, GRID_W, heads_dev, HEAD_DIM)
    scores = (
        jnp.einsum("rqhd,rnhd->hrqn", q_grid, key_band, preferred_element_type=jnp.float32)
        * score_scale
        + offset_terms
    )
    ctx_count = ctx_pairs.shape[0]
    ctx_keys_all = ctx_pairs[:, :col_width].reshape(ctx_count, heads_dev, HEAD_DIM)
    ctx_values_all = ctx_pairs[:, col_width:].reshape(ctx_count, heads_dev, HEAD_DIM)
    ctx_scores = (
        jnp.einsum("rqhd,nhd->hrqn", q_grid, ctx_keys_all, preferred_element_type=jnp.float32)
        * score_scale
    )
    row_max = jnp.maximum(jnp.max(scores, axis=3), jnp.max(ctx_scores, axis=3))
    local_exp = jnp.exp(scores - row_max[..., None])
    ctx_exp = jnp.exp(ctx_scores - row_max[..., None])
    denominator = jnp.sum(local_exp, axis=3) + jnp.sum(ctx_exp, axis=3)
    local_weights = (local_exp / denominator[..., None]).astype(jnp.bfloat16)
    ctx_weights = (ctx_exp / denominator[..., None]).astype(jnp.bfloat16)
    combined = jnp.einsum(
        "hrqn,rnhd->rqhd", local_weights, value_band, preferred_element_type=jnp.float32
    ) + jnp.einsum(
        "hrqn,nhd->rqhd", ctx_weights, ctx_values_all, preferred_element_type=jnp.float32
    )
    attended = combined.astype(jnp.bfloat16).reshape(local_rows * GRID_W, col_width)
    partial_value = jnp.dot(attended, out_weight, preferred_element_type=jnp.float32)
    branch = lax.psum(partial_value.astype(jnp.bfloat16), "tp").astype(jnp.float32)
    return (latent.astype(jnp.float32) + gate_vec[0] * branch).astype(jnp.bfloat16)


MESH = pl.DeviceIdType.MESH
MASKED = -1e30
F32 = jnp.float32
BF16 = jnp.bfloat16


def fused_kernel(
    n_sp,
    n_tp,
    latent,
    context,
    shift_w,
    scale_w,
    gate_w,
    query_w,
    key_w,
    value_w,
    out_w,
    cond,
    ctx_cond,
    norm_gain,
    query_gain,
    key_gain,
    bias_in,
    out,
    x_in,
    x_norm,
    hid,
    w_mod,
    w_qkv,
    w_out,
    mod_sp,
    mod_tp,
    q_stage,
    k_stage,
    v_stage,
    ck_stage,
    cv_stage,
    q_all,
    k_all,
    v_all,
    ctx_k,
    ctx_v,
    bias_pad,
    bias_lines,
    table,
    att_slab,
    att,
    local_sem,
    mod_send,
    mod_recv,
    modt_send,
    modt_recv,
    pair_send,
    pair_recv,
    halo_send,
    halo_recv,
    ctx_send,
    ctx_recv,
    wo_send,
    wo_recv,
    att_send,
    att_recv,
):
    me_s, me_t = lax.axis_index("sp"), lax.axis_index("tp")
    rows, d = latent.shape
    c_rows = context.shape[0]
    width = key_w.shape[1]
    heads = width // HEAD_DIM
    block = shift_w.shape[1]
    l_rows = rows // GRID_W
    halo = WIN_ROWS // 2
    win = WIN_ROWS * GRID_W
    core = lax.rem(me_t, 2)
    chip = lax.div(me_t, 2)
    partner = me_t + 1 - 2 * core
    n_x = n_tp // 2
    side = lax.rem(me_s, 2)
    slab = lax.div(me_s, 2)
    mate = me_s + 1 - 2 * side
    last_slab = n_sp // 2 - 1
    half = width // 2
    half_heads = heads // 2

    def remote(src, dst, send, recv, s, t):
        return pltpu.make_async_remote_copy(
            src_ref=src, dst_ref=dst, send_sem=send, recv_sem=recv,
            device_id=(s, t), device_id_type=MESH,
        )

    barrier = pltpu.get_barrier_semaphore()
    for k in range(1, n_sp):
        pl.semaphore_signal(
            barrier, inc=1, device_id=(lax.rem(me_s + k, n_sp), me_t), device_id_type=MESH
        )
    for k in range(1, n_tp):
        pl.semaphore_signal(
            barrier, inc=1, device_id=(me_s, lax.rem(me_t + k, n_tp)), device_id_type=MESH
        )

    loads = [
        (shift_w, w_mod.at[0]),
        (scale_w, w_mod.at[1]),
        (gate_w, w_mod.at[2]),
        (context, x_in.at[pl.ds(0, c_rows)]),
        (latent, x_in.at[pl.ds(c_rows, rows)]),
        (key_w, w_qkv.at[0]),
        (value_w, w_qkv.at[1]),
        (query_w, w_qkv.at[2]),
        (out_w, w_out.at[me_t]),
    ]
    copies = [pltpu.make_async_copy(a, b, local_sem.at[i]) for i, (a, b) in enumerate(loads)]
    for c in copies[:3]:
        c.start()

    def silu(v):
        return v / (1.0 + jnp.exp(-v))

    two = (16, cond.shape[1])
    row_id = lax.broadcasted_iota(jnp.int32, two, 0)
    act0 = jnp.broadcast_to(silu(cond[...]), two)
    act1 = jnp.broadcast_to(silu(ctx_cond[...]), two)

    def placed(first, second):
        picked = jnp.where(row_id == first, act0, 0.0)
        if second is not None:
            picked = jnp.where(row_id == second, act1, picked)
        return picked.astype(BF16)

    part = jnp.zeros((16, block), F32)
    for i, (first, second) in enumerate(((0, 1), (2, 3), (4, None))):
        copies[i].wait()
        part += jnp.dot(placed(first, second), w_mod[i], preferred_element_type=F32)
    for c in copies[3:]:
        c.start()
    mod_sp[me_s] = part[:8]
    pl.semaphore_wait(barrier, n_sp + n_tp - 2)
    sends = []
    for k in range(1, n_sp):
        peer = lax.rem(me_s + k, n_sp)
        c = remote(
            mod_sp.at[me_s], mod_sp.at[me_s], mod_send.at[k], mod_recv.at[me_s], peer, me_t
        )
        c.start()
        sends.append(c)

    def gather_start(view, sems, source=None):
        send, recv = sems
        mine = view(me_t) if source is None else source
        started = [remote(mine, view(me_t), send(0), recv(me_t), me_s, partner)]
        for k in range(1, n_x):
            far = 2 * lax.rem(chip + k, n_x) + core
            started.append(remote(mine, view(me_t), send(k), recv(me_t), me_s, far))
        for c in reversed(started):
            c.start()
        sends.extend(started)

    def gather_forward(view, sems):
        send, recv = sems
        for k in range(1, n_x):
            came = 2 * lax.rem(chip + n_x - k, n_x) + core
            c = remote(view(came), view(came), send(n_x + k), recv(came), me_s, partner)
            c.wait_recv()
            c.start()
            sends.append(c)

    def gather_finish(view, sems):
        send, recv = sems
        remote(
            view(partner), view(partner), send(0), recv(partner), me_s, partner
        ).wait_recv()
        for k in range(1, n_x):
            came = 2 * lax.rem(chip + n_x - k, n_x) + 1 - core
            remote(
                view(came), view(came), send(n_x + k), recv(came), me_s, partner
            ).wait_recv()

    early = width // 4
    wo_rows = (pl.ds(0, early), pl.ds(early, width - early))

    def wo_view(c):
        return lambda j: w_out.at[j, wo_rows[c]]

    def wo_source(c):
        return out_w.at[wo_rows[c]]

    def wo_sems(c):
        return (lambda k: wo_send.at[c, k]), (lambda k: wo_recv.at[c, k])

    def att_view(h):
        return lambda j: att.at[j, h]

    def att_sems(n):
        return (lambda k: att_send.at[n, k]), (lambda k: att_recv.at[n, k])

    gather_start(wo_view(0), wo_sems(0), wo_source(0))

    copies[3].wait()
    copies[4].wait()
    step = 32

    def norm_rows(i, carry):
        at = pl.ds(pl.multiple_of(i * step, step), step)
        v = x_in[at, :].astype(F32)
        r = lax.rsqrt(jnp.mean(v * v, axis=-1, keepdims=True) + EPS)
        x_norm[at, :] = v * r * norm_gain[...]
        return carry

    lax.fori_loop(0, (rows + c_rows) // step, norm_rows, 0)

    pair = 2 * GRID_W
    q_col = lax.broadcasted_iota(jnp.int32, (GRID_W, pair), 0)
    k_col = lax.broadcasted_iota(jnp.int32, (GRID_W, pair), 1) % GRID_W
    col0 = jnp.clip(q_col - WIN_COLS // 2, 0, GRID_W - WIN_COLS)
    col_open = (k_col >= col0) & (k_col < col0 + WIN_COLS)
    n_pairs = 2 * WIN_ROWS - 2
    bias_pad[...] = jnp.zeros_like(bias_pad)
    for h in range(heads):
        bias_pad[h, : 2 * WIN_ROWS - 1, : 2 * WIN_COLS - 1] = bias_in[:, h, :]
    for h in range(half_heads):
        head = side * half_heads + h
        upper = pltpu.roll(bias_pad[head, 1 : n_pairs + 1, :], GRID_W, 1)
        bias_lines[h, :n_pairs, :] = bias_pad[head, :n_pairs, :] + upper
        for a in range(n_pairs):
            line = jnp.broadcast_to(bias_lines[h, a : a + 1, :], (GRID_W, pair))
            rolled = pltpu.roll(line, pair - (WIN_COLS - 1), 1, stride=1, stride_axis=0)
            table[a, h * GRID_W : (h + 1) * GRID_W, :] = jnp.where(col_open, rolled, MASKED)

    for k in range(1, n_sp):
        peer = lax.rem(me_s + k, n_sp)
        remote(
            mod_sp.at[peer], mod_sp.at[peer], mod_send.at[k], mod_recv.at[peer], peer, me_t
        ).wait_recv()
    total = mod_sp[0]
    for k in range(1, n_sp):
        total = total + mod_sp[k]
    mod_tp[me_t] = total
    for k in range(1, n_tp):
        peer = lax.rem(me_t + k, n_tp)
        c = remote(
            mod_tp.at[me_t], mod_tp.at[me_t], modt_send.at[k], modt_recv.at[me_t], me_s, peer
        )
        c.start()
        sends.append(c)

    gather_start(wo_view(1), wo_sems(1), wo_source(1))

    for k in range(1, n_tp):
        peer = lax.rem(me_t + k, n_tp)
        remote(
            mod_tp.at[peer], mod_tp.at[peer], modt_send.at[k], modt_recv.at[peer], me_s, peer
        ).wait_recv()

    def vec(r):
        return jnp.concatenate([mod_tp[j][r : r + 1, :] for j in range(n_tp)], axis=1)

    def modulate_rows(first, count, shift, scale):
        def body(i, carry):
            at = pl.ds(pl.multiple_of(first + i * step, step), step)
            hid[at, :] = (x_norm[at, :] * scale + shift).astype(BF16)
            return carry

        lax.fori_loop(0, count // step, body, 0)

    modulate_rows(0, c_rows, vec(1), 1.0 + vec(3))
    modulate_rows(c_rows, rows, vec(0), 1.0 + vec(2))

    head_row = lax.broadcasted_iota(jnp.int32, (width, width), 0) // HEAD_DIM
    head_col = lax.broadcasted_iota(jnp.int32, (width, width), 1) // HEAD_DIM
    same_head = (head_row == head_col).astype(F32)

    def head_scale(p, gain):
        mean = jnp.dot(
            p * p, same_head, precision=lax.Precision.HIGHEST, preferred_element_type=F32
        ) * (1.0 / HEAD_DIM)
        wide_gain = jnp.concatenate([gain[...]] * heads, axis=1)
        return (p * lax.rsqrt(mean + EPS) * wide_gain).astype(BF16)

    own = pl.ds(rows + pl.multiple_of(side * rows, rows), rows)
    other = pl.ds(rows + pl.multiple_of((1 - side) * rows, rows), rows)

    def split(stage, value):
        for h in range(2):
            stage[h] = value[:, h * half : (h + 1) * half]

    def trade(index, stage, block_all, at):
        c = remote(
            stage.at[1 - side], block_all.at[at], pair_send.at[index], pair_recv.at[index],
            mate, me_t,
        )
        c.start()
        sends.append(c)
        return c

    def share_ctx(index, stage, block_ctx):
        block_ctx[me_s] = stage[side]
        for k in range(1, n_sp):
            peer = lax.rem(me_s + k, n_sp)
            c = remote(
                stage.at[lax.rem(peer, 2)], block_ctx.at[me_s],
                ctx_send.at[index, k], ctx_recv.at[index, me_s], peer, me_t,
            )
            c.start()
            sends.append(c)

    def halo_copies(index, block_all):
        down = remote(
            block_all.at[pl.ds(rows, rows)], block_all.at[pl.ds(3 * rows, rows)],
            halo_send.at[index, 0], halo_recv.at[index, 0], me_s - 2, me_t,
        )
        up = remote(
            block_all.at[pl.ds(2 * rows, rows)], block_all.at[pl.ds(0, rows)],
            halo_send.at[index, 1], halo_recv.at[index, 1], me_s + 2, me_t,
        )
        return down, up

    def halo_start(mine, index, block_all):
        down, up = halo_copies(index, block_all)
        is_low = side == 0 if mine else side == 1

        @pl.when(is_low & (slab > 0))
        def _():
            down.start()

        @pl.when(jnp.logical_not(is_low) & (slab < last_slab))
        def _():
            up.start()

    copies[5].wait()
    keys = head_scale(jnp.dot(hid[...], w_qkv[0], preferred_element_type=F32), key_gain)
    split(k_stage, keys[c_rows:])
    k_trade = trade(0, k_stage, k_all, own)
    k_all[own, :] = k_stage[side]
    halo_start(True, 0, k_all)
    split(ck_stage, keys[:c_rows])
    share_ctx(0, ck_stage, ctx_k)
    copies[6].wait()
    values = jnp.dot(hid[...], w_qkv[1], preferred_element_type=F32).astype(BF16)
    split(v_stage, values[c_rows:])
    v_trade = trade(1, v_stage, v_all, own)
    v_all[own, :] = v_stage[side]
    halo_start(True, 1, v_all)
    split(cv_stage, values[:c_rows])
    share_ctx(1, cv_stage, ctx_v)
    copies[7].wait()
    queries = head_scale(
        jnp.dot(hid[c_rows:, :], w_qkv[2], preferred_element_type=F32), query_gain
    ) * jnp.asarray(HEAD_DIM ** (-0.5), BF16)
    split(q_stage, queries)
    q_own = pl.ds(pl.multiple_of(side * rows, rows), rows)
    q_trade = trade(2, q_stage, q_all, q_own)
    q_all[q_own, :] = q_stage[side]
    k_trade.wait_recv()
    halo_start(False, 0, k_all)
    v_trade.wait_recv()
    halo_start(False, 1, v_all)
    gather_forward(wo_view(0), wo_sems(0))
    q_trade.wait_recv()

    for index, block_ctx in enumerate((ctx_k, ctx_v)):
        for k in range(1, n_sp):
            peer = lax.rem(me_s + k, n_sp)
            remote(
                block_ctx.at[peer], block_ctx.at[peer],
                ctx_send.at[index, k], ctx_recv.at[index, peer], peer, me_t,
            ).wait_recv()
    for index, block_all in enumerate((k_all, v_all)):
        down, up = halo_copies(index, block_all)

        @pl.when(slab < last_slab)
        def _():
            down.wait_recv()

        @pl.when(slab > 0)
        def _():
            up.wait_recv()

    lane_head = lax.broadcasted_iota(jnp.int32, (GRID_W, half), 1) // HEAD_DIM
    masks = [(lane_head == h).astype(F32) for h in range(half_heads)]
    contract_last = (((1,), (1,)), ((), ()))
    all_ck = ctx_k[...].reshape(n_sp * c_rows, half)
    all_cv = ctx_v[...].reshape(n_sp * c_rows, half)

    def attend(i):
        start = jnp.where(
            slab == 0,
            jnp.maximum(i, halo),
            jnp.where(slab == last_slab, jnp.minimum(i, halo), i),
        )
        if last_slab == 0:
            start = jnp.int32(halo)
        at = pl.ds(pl.multiple_of(start * GRID_W, GRID_W), win)
        row_at = pl.ds(pl.multiple_of(i * GRID_W, GRID_W), GRID_W)
        qi = q_all[row_at, :].astype(F32)
        qs = jnp.concatenate([(qi * m).astype(BF16) for m in masks], axis=0)
        s1 = lax.dot_general(qs, k_all[at, :], contract_last, preferred_element_type=F32)
        first = start - i + WIN_ROWS - 1 - halo
        s1 = s1 + jnp.concatenate([table[first + 2 * m] for m in range(WIN_ROWS // 2)], axis=1)
        s2 = lax.dot_general(qs, all_ck, contract_last, preferred_element_type=F32)
        top = jnp.maximum(
            jnp.max(s1, axis=1, keepdims=True), jnp.max(s2, axis=1, keepdims=True)
        )
        e1 = jnp.exp(s1 - top)
        e2 = jnp.exp(s2 - top)
        inv = 1.0 / (jnp.sum(e1, axis=1, keepdims=True) + jnp.sum(e2, axis=1, keepdims=True))
        o = jnp.dot((e1 * inv).astype(BF16), v_all[at, :], preferred_element_type=F32)
        o = o + jnp.dot((e2 * inv).astype(BF16), all_cv, preferred_element_type=F32)
        picked = o[:GRID_W] * masks[0]
        for h in range(1, half_heads):
            picked = picked + o[h * GRID_W : (h + 1) * GRID_W] * masks[h]
        return picked.astype(BF16)

    for i in range(l_rows):
        att_slab[i * GRID_W : (i + 1) * GRID_W, :] = attend((1 - side) * l_rows + i)
    back = remote(
        att_slab, att.at[me_t, side], pair_send.at[3], pair_recv.at[3], mate, me_t
    )
    back.start()
    sends.append(back)
    for i in range(l_rows):
        att[me_t, side, i * GRID_W : (i + 1) * GRID_W, :] = attend(side * l_rows + i)

    back_in = remote(
        att_slab, att.at[me_t, 1 - side], pair_send.at[3], pair_recv.at[3], mate, me_t
    )
    first, second = att_view(side), att_view(1 - side)
    gather_start(first, att_sems(0))
    back_in.wait_recv()
    gather_start(second, att_sems(1))
    gather_forward(first, att_sems(0))
    gather_forward(wo_view(1), wo_sems(1))
    gather_forward(second, att_sems(1))
    copies[8].wait()
    gather_finish(wo_view(0), wo_sems(0))
    gather_finish(wo_view(1), wo_sems(1))
    gather_finish(first, att_sems(0))
    gather_finish(second, att_sems(1))
    gate = vec(4)
    cols = 512
    for n in range(d // cols):
        at = slice(n * cols, (n + 1) * cols)
        branch = jnp.zeros((rows, cols), F32)
        for j in range(n_tp):
            branch = branch + jnp.dot(
                jnp.concatenate([att[j, 0], att[j, 1]], axis=1),
                w_out[j, :, at],
                preferred_element_type=F32,
            ).astype(BF16).astype(F32)
        base = x_in[c_rows:, at].astype(F32)
        out[:, at] = (base + gate[:, at] * branch).astype(BF16)

    for c in sends:
        c.wait_send()
    for index, block_all in enumerate((k_all, v_all)):
        down, up = halo_copies(index, block_all)

        @pl.when(slab > 0)
        def _():
            down.wait_send()

        @pl.when(slab < last_slab)
        def _():
            up.wait_send()


def per_device(
    latent,
    context,
    condition,
    ctx_condition,
    shift_weight,
    scale_weight,
    gate_weight,
    norm_gain,
    query_weight,
    key_weight,
    value_weight,
    query_gain,
    key_gain,
    offset_bias,
    out_weight,
):
    n_sp, n_tp = lax.axis_size("sp"), lax.axis_size("tp")
    rows, d = latent.shape
    c_rows = context.shape[0]
    width = key_weight.shape[1]
    heads = width // HEAD_DIM
    block = shift_weight.shape[1]
    n_pairs = 2 * WIN_ROWS - 2
    half = width // 2
    half_heads = heads // 2
    any_spec = pl.BlockSpec(memory_space=pl.ANY)
    vmem_spec = pl.BlockSpec(memory_space=pltpu.VMEM)
    dma = pltpu.SemaphoreType.DMA
    return pl.pallas_call(
        functools.partial(fused_kernel, n_sp, n_tp),
        out_shape=pltpu.VMEM((rows, d), BF16),
        in_specs=[any_spec] * 9 + [vmem_spec] * 6,
        out_specs=vmem_spec,
        scratch_shapes=[
            pltpu.VMEM((rows + c_rows, d), BF16),
            pltpu.VMEM((rows + c_rows, d), F32),
            pltpu.VMEM((rows + c_rows, d), BF16),
            pltpu.VMEM((3, shift_weight.shape[0], block), BF16),
            pltpu.VMEM((3, d, width), BF16),
            pltpu.VMEM((n_tp, width, d), BF16),
            pltpu.VMEM((n_sp, 8, block), F32),
            pltpu.VMEM((n_tp, 8, block), F32),
            pltpu.VMEM((2, rows, half), BF16),
            pltpu.VMEM((2, rows, half), BF16),
            pltpu.VMEM((2, rows, half), BF16),
            pltpu.VMEM((2, c_rows, half), BF16),
            pltpu.VMEM((2, c_rows, half), BF16),
            pltpu.VMEM((2 * rows, half), BF16),
            pltpu.VMEM((4 * rows, half), BF16),
            pltpu.VMEM((4 * rows, half), BF16),
            pltpu.VMEM((n_sp, c_rows, half), BF16),
            pltpu.VMEM((n_sp, c_rows, half), BF16),
            pltpu.VMEM((heads, 2 * WIN_ROWS, 2 * GRID_W), F32),
            pltpu.VMEM((half_heads, 2 * WIN_ROWS, 2 * GRID_W), F32),
            pltpu.VMEM((n_pairs, half_heads * GRID_W, 2 * GRID_W), F32),
            pltpu.VMEM((rows, half), BF16),
            pltpu.VMEM((n_tp, 2, rows, half), BF16),
            dma((9,)),
            dma((n_sp,)),
            dma((n_sp,)),
            dma((n_tp,)),
            dma((n_tp,)),
            dma((4,)),
            dma((4,)),
            dma((2, 2)),
            dma((2, 2)),
            dma((2, n_sp)),
            dma((2, n_sp)),
            dma((2, n_tp)),
            dma((2, n_tp)),
            dma((2, n_tp)),
            dma((2, n_tp)),
        ],
        compiler_params=pltpu.CompilerParams(collective_id=0, has_side_effects=True),
        name="fused_block",
    )(
        latent,
        context,
        shift_weight,
        scale_weight,
        gate_weight,
        query_weight,
        key_weight,
        value_weight,
        out_weight,
        condition.reshape(1, -1),
        ctx_condition.reshape(1, -1),
        norm_gain.reshape(1, -1),
        query_gain.reshape(1, -1),
        key_gain.reshape(1, -1),
        offset_bias.transpose(1, 0, 2),
    )


def fused_fits(latent, context, condition, query_weight, n_sp, n_tp):
    rows, c_rows = latent.shape[0] // n_sp, context.shape[0] // n_sp
    width = query_weight.shape[1] // n_tp
    return (
        rows == WIN_ROWS // 2 * GRID_W
        and c_rows % 32 == 0
        and condition.shape[0] // n_sp % 128 == 0
        and width % 256 == 0
        and n_tp % 2 == 0
        and n_sp % 2 == 0
    )


def solution(mesh):
    in_specs = (
        P("sp", None),
        P("sp", None),
        P("sp"),
        P("sp"),
        P("sp", "tp"),
        P("sp", "tp"),
        P("sp", "tp"),
        P(),
        P(None, "tp"),
        P(None, "tp"),
        P(None, "tp"),
        P(),
        P(),
        P("tp", None, None),
        P("tp", None),
    )
    out_specs = P("sp", None)

    def step(latent, context, condition, ctx_condition, *rest):
        n_sp, n_tp = mesh.shape["sp"], mesh.shape["tp"]
        fits = fused_fits(latent, context, condition, rest[4], n_sp, n_tp)
        body = per_device if fits else per_device_plain
        return jax.shard_map(
            body, mesh=mesh, in_specs=in_specs, out_specs=out_specs, check_vma=False
        )(latent, context, condition, ctx_condition, *rest)

    return step
```

```python
import functools

import jax
import jax.numpy as jnp
from jax import lax
from jax.experimental import pallas as pl
from jax.experimental.pallas import tpu as pltpu
from jax.sharding import PartitionSpec as P

HEAD_DIM = 64
GRID_W = 64
WIN_ROWS = 8
WIN_COLS = 16


EPS = 1e-06


def extended(x, sides, width):
    for axis, dim in sides:
        count, length = (lax.axis_size(axis), x.shape[dim])
        up = [(i, (i + 1) % count) for i in range(count - 1)]
        down = [(j, i) for i, j in up]
        last = lax.slice_in_dim(x, length - width, length, axis=dim)
        initial = lax.slice_in_dim(x, 0, width, axis=dim)
        before = lax.ppermute(last, axis, up)
        after = lax.ppermute(initial, axis, down)
        x = jnp.concatenate([before, x, after], axis=dim)
    return x


def modulate(rows_in, norm_gain, shift_vec, scale_vec):
    values = rows_in.astype(jnp.float32)
    normed = values * lax.rsqrt(jnp.mean(values * values, axis=-1, keepdims=True) + EPS)
    return (normed * norm_gain * (1.0 + scale_vec) + shift_vec).astype(jnp.bfloat16)


def head_norm(projected, head_gain):
    row_count = projected.shape[0]
    split_heads = projected.reshape(row_count, -1, head_gain.shape[0])
    normed = split_heads * lax.rsqrt(
        jnp.mean(split_heads * split_heads, axis=-1, keepdims=True) + EPS
    )
    return (normed * head_gain).astype(jnp.bfloat16).reshape(row_count, -1)


def per_device_plain(
    latent,
    context,
    condition,
    ctx_condition,
    shift_weight,
    scale_weight,
    gate_weight,
    norm_gain,
    query_weight,
    key_weight,
    value_weight,
    query_gain,
    key_gain,
    offset_bias,
    out_weight,
):
    activations = jax.nn.silu(jnp.stack([condition, ctx_condition])).astype(jnp.bfloat16)
    part_shift = jnp.dot(activations, shift_weight, preferred_element_type=jnp.float32)
    part_scale = jnp.dot(activations, scale_weight, preferred_element_type=jnp.float32)
    part_gate = jnp.dot(activations[:1], gate_weight, preferred_element_type=jnp.float32)
    block_cols = shift_weight.shape[1]
    first_col = lax.axis_index("tp") * block_cols

    def spread(piece_part):
        padded_vec = jnp.zeros((piece_part.shape[0], block_cols * lax.axis_size("tp")), jnp.float32)
        return lax.dynamic_update_slice_in_dim(padded_vec, piece_part, first_col, 1)

    shift_vec, scale_vec, gate_vec = lax.psum(
        (spread(part_shift), spread(part_scale), spread(part_gate)), ("sp", "tp")
    )
    hidden = modulate(latent, norm_gain, shift_vec[0], scale_vec[0])
    queries = head_norm(
        jnp.dot(hidden, query_weight, preferred_element_type=jnp.float32), query_gain
    )
    keys_lat = head_norm(jnp.dot(hidden, key_weight, preferred_element_type=jnp.float32), key_gain)
    values_lat = jnp.dot(hidden, value_weight, preferred_element_type=jnp.float32).astype(
        jnp.bfloat16
    )
    ctx_hidden = modulate(
        lax.all_gather(context, "sp", axis=0, tiled=True), norm_gain, shift_vec[1], scale_vec[1]
    )
    ctx_keys = head_norm(
        jnp.dot(ctx_hidden, key_weight, preferred_element_type=jnp.float32), key_gain
    )
    ctx_values = jnp.dot(ctx_hidden, value_weight, preferred_element_type=jnp.float32).astype(
        jnp.bfloat16
    )
    ctx_pairs = jnp.concatenate([ctx_keys, ctx_values], axis=1)
    col_width = keys_lat.shape[1]
    heads_dev = col_width // HEAD_DIM
    local_rows = keys_lat.shape[0] // GRID_W
    halo_rows = WIN_ROWS // 2
    window_keys = WIN_ROWS * GRID_W
    key_value = jnp.concatenate([keys_lat, values_lat], axis=1).reshape(
        local_rows, GRID_W, 2 * col_width
    )
    padded = extended(key_value, (("sp", 0),), halo_rows)
    first_row = lax.axis_index("sp") * local_rows
    total_rows = local_rows * lax.axis_size("sp")
    global_rows = first_row + jnp.arange(local_rows, dtype=jnp.int32)
    band_start = jnp.clip(global_rows - halo_rows, 0, total_rows - WIN_ROWS)
    band_global = band_start[:, None] + jnp.arange(WIN_ROWS, dtype=jnp.int32)[None, :]
    banded = jnp.take(padded, band_global - first_row + halo_rows, axis=0)
    key_band = banded[..., :col_width].reshape(local_rows, window_keys, heads_dev, HEAD_DIM)
    value_band = banded[..., col_width:].reshape(local_rows, window_keys, heads_dev, HEAD_DIM)
    row_steps = band_global - global_rows[:, None] + WIN_ROWS - 1
    row_hot = (
        row_steps[:, :, None] == jnp.arange(2 * WIN_ROWS - 1, dtype=jnp.int32)[None, None, :]
    ).astype(jnp.float32)
    column_ids = jnp.arange(GRID_W, dtype=jnp.int32)
    col_steps = (
        jnp.clip(column_ids[None, :] - column_ids[:, None], 1 - WIN_COLS, WIN_COLS - 1)
        + WIN_COLS
        - 1
    )
    col_hot = (
        col_steps[:, :, None] == jnp.arange(2 * WIN_COLS - 1, dtype=jnp.int32)[None, None, :]
    ).astype(jnp.float32)
    col_start = jnp.clip(column_ids - WIN_COLS // 2, 0, GRID_W - WIN_COLS)
    col_open = (column_ids[None, :] >= col_start[:, None]) & (
        column_ids[None, :] < col_start[:, None] + WIN_COLS
    )
    col_table = jnp.einsum("hab,qkb->haqk", offset_bias, col_hot, precision=lax.Precision.HIGHEST)
    col_table = jnp.where(col_open[None, None, :, :], col_table, -jnp.inf)
    offset_terms = jnp.einsum(
        "rja,haqk->hrqjk",
        row_hot,
        jnp.where(col_open[None, None], col_table, 0.0),
        precision=lax.Precision.HIGHEST,
    )
    offset_terms = jnp.where(col_open[None, None, :, None, :], offset_terms, -jnp.inf)
    offset_terms = offset_terms.reshape(heads_dev, local_rows, GRID_W, window_keys)
    score_scale = HEAD_DIM ** (-0.5)
    q_grid = queries.reshape(local_rows, GRID_W, heads_dev, HEAD_DIM)
    scores = (
        jnp.einsum("rqhd,rnhd->hrqn", q_grid, key_band, preferred_element_type=jnp.float32)
        * score_scale
        + offset_terms
    )
    ctx_count = ctx_pairs.shape[0]
    ctx_keys_all = ctx_pairs[:, :col_width].reshape(ctx_count, heads_dev, HEAD_DIM)
    ctx_values_all = ctx_pairs[:, col_width:].reshape(ctx_count, heads_dev, HEAD_DIM)
    ctx_scores = (
        jnp.einsum("rqhd,nhd->hrqn", q_grid, ctx_keys_all, preferred_element_type=jnp.float32)
        * score_scale
    )
    row_max = jnp.maximum(jnp.max(scores, axis=3), jnp.max(ctx_scores, axis=3))
    local_exp = jnp.exp(scores - row_max[..., None])
    ctx_exp = jnp.exp(ctx_scores - row_max[..., None])
    denominator = jnp.sum(local_exp, axis=3) + jnp.sum(ctx_exp, axis=3)
    local_weights = (local_exp / denominator[..., None]).astype(jnp.bfloat16)
    ctx_weights = (ctx_exp / denominator[..., None]).astype(jnp.bfloat16)
    combined = jnp.einsum(
        "hrqn,rnhd->rqhd", local_weights, value_band, preferred_element_type=jnp.float32
    ) + jnp.einsum(
        "hrqn,nhd->rqhd", ctx_weights, ctx_values_all, preferred_element_type=jnp.float32
    )
    attended = combined.astype(jnp.bfloat16).reshape(local_rows * GRID_W, col_width)
    partial_value = jnp.dot(attended, out_weight, preferred_element_type=jnp.float32)
    branch = lax.psum(partial_value.astype(jnp.bfloat16), "tp").astype(jnp.float32)
    return (latent.astype(jnp.float32) + gate_vec[0] * branch).astype(jnp.bfloat16)


MESH = pl.DeviceIdType.MESH
MASKED = -1e30
F32 = jnp.float32
BF16 = jnp.bfloat16


def fused_kernel(
    n_sp,
    n_tp,
    latent,
    context,
    shift_w,
    scale_w,
    gate_w,
    query_w,
    key_w,
    value_w,
    out_w,
    cond,
    ctx_cond,
    norm_gain,
    query_gain,
    key_gain,
    bias_in,
    out,
    x_in,
    x_norm,
    hid,
    w_mod,
    w_qkv,
    w_out,
    mod_sp,
    mod_tp,
    q_stage,
    k_stage,
    v_stage,
    ck_stage,
    cv_stage,
    q_all,
    k_all,
    v_all,
    ctx_k,
    ctx_v,
    bias_pad,
    bias_lines,
    table,
    att_slab,
    att,
    local_sem,
    mod_send,
    mod_recv,
    modt_send,
    modt_recv,
    pair_send,
    pair_recv,
    halo_send,
    halo_recv,
    ctx_send,
    ctx_recv,
    wo_send,
    wo_recv,
    att_send,
    att_recv,
):
    me_s, me_t = lax.axis_index("sp"), lax.axis_index("tp")
    rows, d = latent.shape
    c_rows = context.shape[0]
    width = key_w.shape[1]
    heads = width // HEAD_DIM
    block = shift_w.shape[1]
    l_rows = rows // GRID_W
    halo = WIN_ROWS // 2
    win = WIN_ROWS * GRID_W
    core = lax.rem(me_t, 2)
    chip = lax.div(me_t, 2)
    partner = me_t + 1 - 2 * core
    n_x = n_tp // 2
    side = lax.rem(me_s, 2)
    slab = lax.div(me_s, 2)
    mate = me_s + 1 - 2 * side
    last_slab = n_sp // 2 - 1
    half = width // 2
    half_heads = heads // 2

    def remote(src, dst, send, recv, s, t):
        return pltpu.make_async_remote_copy(
            src_ref=src, dst_ref=dst, send_sem=send, recv_sem=recv,
            device_id=(s, t), device_id_type=MESH,
        )

    barrier = pltpu.get_barrier_semaphore()
    for k in range(1, n_sp):
        pl.semaphore_signal(
            barrier, inc=1, device_id=(lax.rem(me_s + k, n_sp), me_t), device_id_type=MESH
        )
    for k in range(1, n_tp):
        pl.semaphore_signal(
            barrier, inc=1, device_id=(me_s, lax.rem(me_t + k, n_tp)), device_id_type=MESH
        )

    loads = [
        (shift_w, w_mod.at[0]),
        (scale_w, w_mod.at[1]),
        (gate_w, w_mod.at[2]),
        (context, x_in.at[pl.ds(0, c_rows)]),
        (latent, x_in.at[pl.ds(c_rows, rows)]),
        (key_w, w_qkv.at[0]),
        (value_w, w_qkv.at[1]),
        (query_w, w_qkv.at[2]),
        (out_w, w_out.at[me_t]),
    ]
    copies = [pltpu.make_async_copy(a, b, local_sem.at[i]) for i, (a, b) in enumerate(loads)]
    for c in copies[:3]:
        c.start()

    def silu(v):
        return v / (1.0 + jnp.exp(-v))

    two = (16, cond.shape[1])
    row_id = lax.broadcasted_iota(jnp.int32, two, 0)
    act0 = jnp.broadcast_to(silu(cond[...]), two)
    act1 = jnp.broadcast_to(silu(ctx_cond[...]), two)

    def placed(first, second):
        picked = jnp.where(row_id == first, act0, 0.0)
        if second is not None:
            picked = jnp.where(row_id == second, act1, picked)
        return picked.astype(BF16)

    part = jnp.zeros((16, block), F32)
    for i, (first, second) in enumerate(((0, 1), (2, 3), (4, None))):
        copies[i].wait()
        part += jnp.dot(placed(first, second), w_mod[i], preferred_element_type=F32)
    for c in copies[3:]:
        c.start()
    mod_sp[me_s] = part[:8]
    pl.semaphore_wait(barrier, n_sp + n_tp - 2)
    sends = []
    for k in range(1, n_sp):
        peer = lax.rem(me_s + k, n_sp)
        c = remote(
            mod_sp.at[me_s], mod_sp.at[me_s], mod_send.at[k], mod_recv.at[me_s], peer, me_t
        )
        c.start()
        sends.append(c)

    def gather_start(view, sems, source=None):
        send, recv = sems
        mine = view(me_t) if source is None else source
        started = [remote(mine, view(me_t), send(0), recv(me_t), me_s, partner)]
        for k in range(1, n_x):
            far = 2 * lax.rem(chip + k, n_x) + core
            started.append(remote(mine, view(me_t), send(k), recv(me_t), me_s, far))
        for c in reversed(started):
            c.start()
        sends.extend(started)

    def gather_forward(view, sems):
        send, recv = sems
        for k in range(1, n_x):
            came = 2 * lax.rem(chip + n_x - k, n_x) + core
            c = remote(view(came), view(came), send(n_x + k), recv(came), me_s, partner)
            c.wait_recv()
            c.start()
            sends.append(c)

    def gather_finish(view, sems):
        send, recv = sems
        remote(
            view(partner), view(partner), send(0), recv(partner), me_s, partner
        ).wait_recv()
        for k in range(1, n_x):
            came = 2 * lax.rem(chip + n_x - k, n_x) + 1 - core
            remote(
                view(came), view(came), send(n_x + k), recv(came), me_s, partner
            ).wait_recv()

    early = width // 4
    later = (width - early) // 2
    wo_rows = (pl.ds(0, early), pl.ds(early, later), pl.ds(early + later, later))

    def wo_view(c):
        return lambda j: w_out.at[j, wo_rows[c]]

    def wo_source(c):
        return out_w.at[wo_rows[c]]

    def wo_sems(c):
        return (lambda k: wo_send.at[c, k]), (lambda k: wo_recv.at[c, k])

    def att_view(h):
        return lambda j: att.at[j, h]

    def att_sems(n):
        return (lambda k: att_send.at[n, k]), (lambda k: att_recv.at[n, k])

    gather_start(wo_view(0), wo_sems(0), wo_source(0))

    copies[3].wait()
    copies[4].wait()
    step = 32

    def norm_rows(i, carry):
        at = pl.ds(pl.multiple_of(i * step, step), step)
        v = x_in[at, :].astype(F32)
        r = lax.rsqrt(jnp.mean(v * v, axis=-1, keepdims=True) + EPS)
        x_norm[at, :] = v * r * norm_gain[...]
        return carry

    lax.fori_loop(0, (rows + c_rows) // step, norm_rows, 0)

    pair = 2 * GRID_W
    q_col = lax.broadcasted_iota(jnp.int32, (GRID_W, pair), 0)
    k_col = lax.broadcasted_iota(jnp.int32, (GRID_W, pair), 1) % GRID_W
    col0 = jnp.clip(q_col - WIN_COLS // 2, 0, GRID_W - WIN_COLS)
    col_open = (k_col >= col0) & (k_col < col0 + WIN_COLS)
    n_pairs = 2 * WIN_ROWS - 2
    bias_pad[...] = jnp.zeros_like(bias_pad)
    for h in range(heads):
        bias_pad[h, : 2 * WIN_ROWS - 1, : 2 * WIN_COLS - 1] = bias_in[:, h, :]
    for h in range(half_heads):
        head = side * half_heads + h
        upper = pltpu.roll(bias_pad[head, 1 : n_pairs + 1, :], GRID_W, 1)
        bias_lines[h, :n_pairs, :] = bias_pad[head, :n_pairs, :] + upper
        for a in range(n_pairs):
            line = jnp.broadcast_to(bias_lines[h, a : a + 1, :], (GRID_W, pair))
            rolled = pltpu.roll(line, pair - (WIN_COLS - 1), 1, stride=1, stride_axis=0)
            table[a, h * GRID_W : (h + 1) * GRID_W, :] = jnp.where(col_open, rolled, MASKED)

    for k in range(1, n_sp):
        peer = lax.rem(me_s + k, n_sp)
        remote(
            mod_sp.at[peer], mod_sp.at[peer], mod_send.at[k], mod_recv.at[peer], peer, me_t
        ).wait_recv()
    total = mod_sp[0]
    for k in range(1, n_sp):
        total = total + mod_sp[k]
    mod_tp[me_t] = total
    for k in range(1, n_tp):
        peer = lax.rem(me_t + k, n_tp)
        c = remote(
            mod_tp.at[me_t], mod_tp.at[me_t], modt_send.at[k], modt_recv.at[me_t], me_s, peer
        )
        c.start()
        sends.append(c)

    gather_start(wo_view(1), wo_sems(1), wo_source(1))
    gather_start(wo_view(2), wo_sems(2), wo_source(2))

    for k in range(1, n_tp):
        peer = lax.rem(me_t + k, n_tp)
        remote(
            mod_tp.at[peer], mod_tp.at[peer], modt_send.at[k], modt_recv.at[peer], me_s, peer
        ).wait_recv()

    def vec(r):
        return jnp.concatenate([mod_tp[j][r : r + 1, :] for j in range(n_tp)], axis=1)

    def modulate_rows(first, count, shift, scale):
        def body(i, carry):
            at = pl.ds(pl.multiple_of(first + i * step, step), step)
            hid[at, :] = (x_norm[at, :] * scale + shift).astype(BF16)
            return carry

        lax.fori_loop(0, count // step, body, 0)

    modulate_rows(0, c_rows, vec(1), 1.0 + vec(3))
    modulate_rows(c_rows, rows, vec(0), 1.0 + vec(2))

    head_row = lax.broadcasted_iota(jnp.int32, (width, width), 0) // HEAD_DIM
    head_col = lax.broadcasted_iota(jnp.int32, (width, width), 1) // HEAD_DIM
    same_head = (head_row == head_col).astype(F32)

    def head_scale(p, gain):
        mean = jnp.dot(
            p * p, same_head, precision=lax.Precision.HIGHEST, preferred_element_type=F32
        ) * (1.0 / HEAD_DIM)
        wide_gain = jnp.concatenate([gain[...]] * heads, axis=1)
        return (p * lax.rsqrt(mean + EPS) * wide_gain).astype(BF16)

    own = pl.ds(rows + pl.multiple_of(side * rows, rows), rows)
    other = pl.ds(rows + pl.multiple_of((1 - side) * rows, rows), rows)

    def split(stage, value):
        for h in range(2):
            stage[h] = value[:, h * half : (h + 1) * half]

    def trade(index, stage, block_all, at):
        c = remote(
            stage.at[1 - side], block_all.at[at], pair_send.at[index], pair_recv.at[index],
            mate, me_t,
        )
        c.start()
        sends.append(c)
        return c

    def share_ctx(index, stage, block_ctx):
        block_ctx[me_s] = stage[side]
        for k in range(1, n_sp):
            peer = lax.rem(me_s + k, n_sp)
            c = remote(
                stage.at[lax.rem(peer, 2)], block_ctx.at[me_s],
                ctx_send.at[index, k], ctx_recv.at[index, me_s], peer, me_t,
            )
            c.start()
            sends.append(c)

    def halo_copies(index, block_all):
        down = remote(
            block_all.at[pl.ds(rows, rows)], block_all.at[pl.ds(3 * rows, rows)],
            halo_send.at[index, 0], halo_recv.at[index, 0], me_s - 2, me_t,
        )
        up = remote(
            block_all.at[pl.ds(2 * rows, rows)], block_all.at[pl.ds(0, rows)],
            halo_send.at[index, 1], halo_recv.at[index, 1], me_s + 2, me_t,
        )
        return down, up

    def halo_start(mine, index, block_all):
        down, up = halo_copies(index, block_all)
        is_low = side == 0 if mine else side == 1

        @pl.when(is_low & (slab > 0))
        def _():
            down.start()

        @pl.when(jnp.logical_not(is_low) & (slab < last_slab))
        def _():
            up.start()

    copies[5].wait()
    keys = head_scale(jnp.dot(hid[...], w_qkv[0], preferred_element_type=F32), key_gain)
    split(k_stage, keys[c_rows:])
    k_trade = trade(0, k_stage, k_all, own)
    k_all[own, :] = k_stage[side]
    halo_start(True, 0, k_all)
    split(ck_stage, keys[:c_rows])
    share_ctx(0, ck_stage, ctx_k)
    copies[6].wait()
    values = jnp.dot(hid[...], w_qkv[1], preferred_element_type=F32).astype(BF16)
    split(v_stage, values[c_rows:])
    v_trade = trade(1, v_stage, v_all, own)
    v_all[own, :] = v_stage[side]
    halo_start(True, 1, v_all)
    split(cv_stage, values[:c_rows])
    share_ctx(1, cv_stage, ctx_v)
    copies[7].wait()
    queries = head_scale(
        jnp.dot(hid[c_rows:, :], w_qkv[2], preferred_element_type=F32), query_gain
    ) * jnp.asarray(HEAD_DIM ** (-0.5), BF16)
    split(q_stage, queries)
    q_own = pl.ds(pl.multiple_of(side * rows, rows), rows)
    q_trade = trade(2, q_stage, q_all, q_own)
    q_all[q_own, :] = q_stage[side]
    k_trade.wait_recv()
    halo_start(False, 0, k_all)
    v_trade.wait_recv()
    halo_start(False, 1, v_all)
    gather_forward(wo_view(0), wo_sems(0))
    q_trade.wait_recv()

    for index, block_ctx in enumerate((ctx_k, ctx_v)):
        for k in range(1, n_sp):
            peer = lax.rem(me_s + k, n_sp)
            remote(
                block_ctx.at[peer], block_ctx.at[peer],
                ctx_send.at[index, k], ctx_recv.at[index, peer], peer, me_t,
            ).wait_recv()
    for index, block_all in enumerate((k_all, v_all)):
        down, up = halo_copies(index, block_all)

        @pl.when(slab < last_slab)
        def _():
            down.wait_recv()

        @pl.when(slab > 0)
        def _():
            up.wait_recv()

    lane_head = lax.broadcasted_iota(jnp.int32, (GRID_W, half), 1) // HEAD_DIM
    masks = [(lane_head == h).astype(F32) for h in range(half_heads)]
    contract_last = (((1,), (1,)), ((), ()))
    all_ck = ctx_k[...].reshape(n_sp * c_rows, half)
    all_cv = ctx_v[...].reshape(n_sp * c_rows, half)

    def attend(i):
        start = jnp.where(
            slab == 0,
            jnp.maximum(i, halo),
            jnp.where(slab == last_slab, jnp.minimum(i, halo), i),
        )
        if last_slab == 0:
            start = jnp.int32(halo)
        at = pl.ds(pl.multiple_of(start * GRID_W, GRID_W), win)
        row_at = pl.ds(pl.multiple_of(i * GRID_W, GRID_W), GRID_W)
        qi = q_all[row_at, :].astype(F32)
        qs = jnp.concatenate([(qi * m).astype(BF16) for m in masks], axis=0)
        s1 = lax.dot_general(qs, k_all[at, :], contract_last, preferred_element_type=F32)
        first = start - i + WIN_ROWS - 1 - halo
        s1 = s1 + jnp.concatenate([table[first + 2 * m] for m in range(WIN_ROWS // 2)], axis=1)
        s2 = lax.dot_general(qs, all_ck, contract_last, preferred_element_type=F32)
        top = jnp.maximum(
            jnp.max(s1, axis=1, keepdims=True), jnp.max(s2, axis=1, keepdims=True)
        )
        e1 = jnp.exp(s1 - top)
        e2 = jnp.exp(s2 - top)
        inv = 1.0 / (jnp.sum(e1, axis=1, keepdims=True) + jnp.sum(e2, axis=1, keepdims=True))
        o = jnp.dot((e1 * inv).astype(BF16), v_all[at, :], preferred_element_type=F32)
        o = o + jnp.dot((e2 * inv).astype(BF16), all_cv, preferred_element_type=F32)
        picked = o[:GRID_W] * masks[0]
        for h in range(1, half_heads):
            picked = picked + o[h * GRID_W : (h + 1) * GRID_W] * masks[h]
        return picked.astype(BF16)

    for i in range(l_rows):
        att_slab[i * GRID_W : (i + 1) * GRID_W, :] = attend((1 - side) * l_rows + i)
    back = remote(
        att_slab, att.at[me_t, side], pair_send.at[3], pair_recv.at[3], mate, me_t
    )
    back.start()
    sends.append(back)
    gather_forward(wo_view(1), wo_sems(1))
    for i in range(l_rows):
        att[me_t, side, i * GRID_W : (i + 1) * GRID_W, :] = attend(side * l_rows + i)

    back_in = remote(
        att_slab, att.at[me_t, 1 - side], pair_send.at[3], pair_recv.at[3], mate, me_t
    )
    first, second = att_view(side), att_view(1 - side)
    gather_start(first, att_sems(0))
    back_in.wait_recv()
    gather_start(second, att_sems(1))
    gather_forward(first, att_sems(0))
    gather_forward(wo_view(2), wo_sems(2))
    gather_forward(second, att_sems(1))
    copies[8].wait()
    gather_finish(wo_view(0), wo_sems(0))
    gather_finish(wo_view(1), wo_sems(1))
    gather_finish(wo_view(2), wo_sems(2))
    gather_finish(first, att_sems(0))
    gather_finish(second, att_sems(1))
    gate = vec(4)
    cols = 512
    for n in range(d // cols):
        at = slice(n * cols, (n + 1) * cols)
        branch = jnp.zeros((rows, cols), F32)
        for j in range(n_tp):
            branch = branch + jnp.dot(
                jnp.concatenate([att[j, 0], att[j, 1]], axis=1),
                w_out[j, :, at],
                preferred_element_type=F32,
            ).astype(BF16).astype(F32)
        base = x_in[c_rows:, at].astype(F32)
        out[:, at] = (base + gate[:, at] * branch).astype(BF16)

    for c in sends:
        c.wait_send()
    for index, block_all in enumerate((k_all, v_all)):
        down, up = halo_copies(index, block_all)

        @pl.when(slab > 0)
        def _():
            down.wait_send()

        @pl.when(slab < last_slab)
        def _():
            up.wait_send()


def per_device(
    latent,
    context,
    condition,
    ctx_condition,
    shift_weight,
    scale_weight,
    gate_weight,
    norm_gain,
    query_weight,
    key_weight,
    value_weight,
    query_gain,
    key_gain,
    offset_bias,
    out_weight,
):
    n_sp, n_tp = lax.axis_size("sp"), lax.axis_size("tp")
    rows, d = latent.shape
    c_rows = context.shape[0]
    width = key_weight.shape[1]
    heads = width // HEAD_DIM
    block = shift_weight.shape[1]
    n_pairs = 2 * WIN_ROWS - 2
    half = width // 2
    half_heads = heads // 2
    any_spec = pl.BlockSpec(memory_space=pl.ANY)
    vmem_spec = pl.BlockSpec(memory_space=pltpu.VMEM)
    dma = pltpu.SemaphoreType.DMA
    return pl.pallas_call(
        functools.partial(fused_kernel, n_sp, n_tp),
        out_shape=pltpu.VMEM((rows, d), BF16),
        in_specs=[any_spec] * 9 + [vmem_spec] * 6,
        out_specs=vmem_spec,
        scratch_shapes=[
            pltpu.VMEM((rows + c_rows, d), BF16),
            pltpu.VMEM((rows + c_rows, d), F32),
            pltpu.VMEM((rows + c_rows, d), BF16),
            pltpu.VMEM((3, shift_weight.shape[0], block), BF16),
            pltpu.VMEM((3, d, width), BF16),
            pltpu.VMEM((n_tp, width, d), BF16),
            pltpu.VMEM((n_sp, 8, block), F32),
            pltpu.VMEM((n_tp, 8, block), F32),
            pltpu.VMEM((2, rows, half), BF16),
            pltpu.VMEM((2, rows, half), BF16),
            pltpu.VMEM((2, rows, half), BF16),
            pltpu.VMEM((2, c_rows, half), BF16),
            pltpu.VMEM((2, c_rows, half), BF16),
            pltpu.VMEM((2 * rows, half), BF16),
            pltpu.VMEM((4 * rows, half), BF16),
            pltpu.VMEM((4 * rows, half), BF16),
            pltpu.VMEM((n_sp, c_rows, half), BF16),
            pltpu.VMEM((n_sp, c_rows, half), BF16),
            pltpu.VMEM((heads, 2 * WIN_ROWS, 2 * GRID_W), F32),
            pltpu.VMEM((half_heads, 2 * WIN_ROWS, 2 * GRID_W), F32),
            pltpu.VMEM((n_pairs, half_heads * GRID_W, 2 * GRID_W), F32),
            pltpu.VMEM((rows, half), BF16),
            pltpu.VMEM((n_tp, 2, rows, half), BF16),
            dma((9,)),
            dma((n_sp,)),
            dma((n_sp,)),
            dma((n_tp,)),
            dma((n_tp,)),
            dma((4,)),
            dma((4,)),
            dma((2, 2)),
            dma((2, 2)),
            dma((2, n_sp)),
            dma((2, n_sp)),
            dma((3, n_tp)),
            dma((3, n_tp)),
            dma((2, n_tp)),
            dma((2, n_tp)),
        ],
        compiler_params=pltpu.CompilerParams(collective_id=0, has_side_effects=True),
        name="fused_block",
    )(
        latent,
        context,
        shift_weight,
        scale_weight,
        gate_weight,
        query_weight,
        key_weight,
        value_weight,
        out_weight,
        condition.reshape(1, -1),
        ctx_condition.reshape(1, -1),
        norm_gain.reshape(1, -1),
        query_gain.reshape(1, -1),
        key_gain.reshape(1, -1),
        offset_bias.transpose(1, 0, 2),
    )


def fused_fits(latent, context, condition, query_weight, n_sp, n_tp):
    rows, c_rows = latent.shape[0] // n_sp, context.shape[0] // n_sp
    width = query_weight.shape[1] // n_tp
    return (
        rows == WIN_ROWS // 2 * GRID_W
        and c_rows % 32 == 0
        and condition.shape[0] // n_sp % 128 == 0
        and width % 256 == 0
        and n_tp % 2 == 0
        and n_sp % 2 == 0
    )


def solution(mesh):
    in_specs = (
        P("sp", None),
        P("sp", None),
        P("sp"),
        P("sp"),
        P("sp", "tp"),
        P("sp", "tp"),
        P("sp", "tp"),
        P(),
        P(None, "tp"),
        P(None, "tp"),
        P(None, "tp"),
        P(),
        P(),
        P("tp", None, None),
        P("tp", None),
    )
    out_specs = P("sp", None)

    def step(latent, context, condition, ctx_condition, *rest):
        n_sp, n_tp = mesh.shape["sp"], mesh.shape["tp"]
        fits = fused_fits(latent, context, condition, rest[4], n_sp, n_tp)
        body = per_device if fits else per_device_plain
        return jax.shard_map(
            body, mesh=mesh, in_specs=in_specs, out_specs=out_specs, check_vma=False
        )(latent, context, condition, ctx_condition, *rest)

    return step
```
